32 devices in a mesh: rep: 2 (over x), fs: 8 (over z, y), tp: 2 (over core).
Axes of the slice: x: 2, y: 2, z: 4, core: 2. Of those that a mesh axis runs over, the one named last changes fastest.
Arguments:
- resid: bfloat16 [16384, 2048], P(('rep', 'fs'), 'tp'), may hold values from -6 to 6
- gain_mix_in: float32 [2048], replicated, may hold values from 0.1 to 1.9
- u_weight: float32 [2048, 1024], P('fs', 'tp'), may hold values from -0.125 to 0.125
- v_weight: float32 [2048, 1024], P('fs', 'tp'), may hold values from -0.125 to 0.125
- u_scale: float32 [1024], P('tp'), may hold values from 0.5 to 2
- v_scale: float32 [1024], P('tp'), may hold values from 0.3 to 3
- v_gain: float32 [1024], P('tp'), may hold values from 0.1 to 1.9
- mix_matrix: float32 [16, 128, 128], P('tp'), may hold values from -0.5 to 0.5
- mix_bias: float32 [16, 128], P('tp'), may hold values from 0.1 to 1.9
- out_weight: float32 [1024, 2048], P('tp', 'fs'), may hold values from -0.1875 to 0.1875
- out_scale: float32 [2048], P('fs'), may hold values from 0.3 to 3
- gain_mix_out: float32 [2048], replicated, may hold values from 0.1 to 1.9
- gain_ffn_in: float32 [2048], replicated, may hold values from 0.1 to 1.9
- up_weight: float32 [2048, 4096], P('fs', 'tp'), may hold values from -0.125 to 0.125
- up_scale: float32 [4096], P('tp'), may hold values from 0.5 to 2
- down_weight: float32 [4096, 2048], P('tp', 'fs'), may hold values from -0.09375 to 0.09375
- down_scale: float32 [2048], P('fs'), may hold values from 0.3 to 3
- gain_ffn_out: float32 [2048], replicated, may hold values from 0.1 to 1.9
Outputs:
- result: bfloat16 [16384, 2048], P(('rep', 'fs'), 'tp')
The draws below stay inside these ranges and needn't reach their ends.
All inputs are finite; a program needn't handle non-finite values.
Results may differ from the reference program's by a relative error of at most 0.013.
Values may be sent and summed in bfloat16 or wider, within the bound.
A program may use at most 128 MiB of HBM per device.

```python
import math
import jax
import jax.numpy as jnp
from jax import lax

D = 2048
A = 1024
GROUPS = 16
FF = 4096
BLOCK = 128
TOKENS = 16384
N_TP = 2


def shard_levels(key, dims, split, smallest, high):
    loudness = 1.0
    for dim, shards_of in split:
        heights = jax.random.uniform(jax.random.fold_in(jax.random.fold_in(key, 6), dim), (shards_of,), jnp.float32, smallest / len(split), high / len(split))
        loudness = loudness * jnp.repeat(jnp.exp(heights), dims[dim] // shards_of).reshape((-1,) + (1,) * (len(dims) - 1 - dim))
    return loudness


def normal_values(own_key, dims, scale, bound, shards=(), kind=jnp.bfloat16):
    loudness = shard_levels(own_key, dims, shards, -0.22, 0.18) if shards else 1.0
    drawn = jax.random.normal(own_key, dims, jnp.float32) * scale * loudness
    return jnp.minimum(jnp.maximum(drawn, -bound), bound).astype(kind)


def setup_inputs(seed: int = 0) -> dict:
    streams_of = jax.random.split(jax.random.key(seed), 19)
    return {
        "resid": normal_values(streams_of[0], (TOKENS, D), 1.0, 6.0, ((0, 16), (1, 2))),
        "gain_mix_in": jnp.clip(1.0 + 0.18 * jax.random.normal(streams_of[1], (D,), jnp.float32), 0.1, 1.9),
        "u_weight": normal_values(streams_of[2], (D, A), D ** -0.5, 0.125, ((0, 8), (1, 2)), jnp.float32),
        "v_weight": normal_values(streams_of[3], (D, A), D ** -0.5, 0.125, ((0, 8), (1, 2)), jnp.float32),
        "u_scale": jnp.clip(jnp.exp(math.log(2.0) - 1.3862944 * jax.random.uniform(streams_of[4], (A,), jnp.float32) ** shard_levels(streams_of[4], (A,), ((0, 2),), -0.2, 0.2)), 0.5, 2.0),
        "v_scale": jnp.clip(jnp.exp(math.log(3.0) - 2.3025851 * jax.random.uniform(streams_of[5], (A,), jnp.float32) ** shard_levels(streams_of[5], (A,), ((0, 2),), -0.2, 0.2)), 0.3, 3.0),
        "v_gain": jnp.clip(1.0 + 0.18 * jax.random.normal(streams_of[6], (A,), jnp.float32), 0.1, 1.9),
        "mix_matrix": normal_values(streams_of[7], (GROUPS, BLOCK, BLOCK), BLOCK ** -0.5, 0.5, ((0, 2),), jnp.float32),
        "mix_bias": jnp.clip(1.0 + 0.18 * jax.random.normal(streams_of[8], (GROUPS, BLOCK), jnp.float32), 0.1, 1.9),
        "out_weight": normal_values(streams_of[9], (A, D), A ** -0.5, 0.1875, ((0, 2), (1, 8)), jnp.float32),
        "out_scale": jnp.clip(jnp.exp(math.log(3.0) - 2.3025851 * jax.random.uniform(streams_of[10], (D,), jnp.float32) ** shard_levels(streams_of[10], (D,), ((0, 8),), -0.2, 0.2)), 0.3, 3.0),
        "gain_mix_out": jnp.clip(1.0 + 0.18 * jax.random.normal(streams_of[11], (D,), jnp.float32), 0.1, 1.9),
        "gain_ffn_in": jnp.clip(1.0 + 0.18 * jax.random.normal(streams_of[12], (D,), jnp.float32), 0.1, 1.9),
        "up_weight": normal_values(streams_of[13], (D, FF), D ** -0.5, 0.125, ((0, 8), (1, 2)), jnp.float32),
        "up_scale": jnp.clip(jnp.exp(math.log(2.0) - 1.3862944 * jax.random.uniform(streams_of[14], (FF,), jnp.float32) ** shard_levels(streams_of[14], (FF,), ((0, 2),), -0.2, 0.2)), 0.5, 2.0),
        "down_weight": normal_values(streams_of[15], (FF, D), FF ** -0.5, 0.09375, ((0, 2), (1, 8)), jnp.float32),
        "down_scale": jnp.clip(jnp.exp(math.log(3.0) - 2.3025851 * jax.random.uniform(streams_of[16], (D,), jnp.float32) ** shard_levels(streams_of[16], (D,), ((0, 8),), -0.2, 0.2)), 0.3, 3.0),
        "gain_ffn_out": jnp.clip(1.0 + 0.18 * jax.random.normal(streams_of[17], (D,), jnp.float32), 0.1, 1.9),
    }


def rms_norm(values, gain):
    power = lax.optimization_barrier(jnp.mean(values * values, axis=-1, keepdims=True))
    return values * lax.rsqrt(power + 1e-06) * gain

def split_sum(left, right, pieces):
    width = left.shape[1] // pieces
    total = jnp.zeros((left.shape[0], right.shape[1]), jnp.float32)
    for index in range(pieces):
        lower = index * width
        partial_value = jnp.dot(left[:, lower:lower + width], right[lower:lower + width], preferred_element_type=jnp.float32)
        rounded = lax.optimization_barrier(partial_value.astype(jnp.bfloat16))
        total = total + rounded.astype(jnp.float32)
    return total

def reference(resid, gain_mix_in, u_weight, v_weight, u_scale, v_scale, v_gain, mix_matrix, mix_bias, out_weight, out_scale, gain_mix_out, gain_ffn_in, up_weight, up_scale, down_weight, down_scale, gain_ffn_out):
    stream = resid.astype(jnp.float32)
    normed = rms_norm(stream, gain_mix_in).astype(jnp.bfloat16)
    u_act = jax.nn.gelu(jnp.dot(normed, u_weight.astype(jnp.bfloat16), preferred_element_type=jnp.float32) * u_scale)
    v_act = jax.nn.gelu(jnp.dot(normed, v_weight.astype(jnp.bfloat16), preferred_element_type=jnp.float32) * v_scale)
    centre = lax.optimization_barrier(jnp.mean(v_act, axis=-1, keepdims=True))
    spread = lax.optimization_barrier(jnp.mean(jnp.square(v_act - centre), axis=-1, keepdims=True))
    v_norm = ((v_act - centre) * lax.rsqrt(spread + 1e-06) * v_gain).astype(jnp.bfloat16)
    tokens = resid.shape[0]
    groups = mix_matrix.shape[0]
    blocks = v_norm.reshape(tokens // BLOCK, BLOCK, groups, A // groups).astype(jnp.float32)
    matrix = mix_matrix.astype(jnp.bfloat16).astype(jnp.float32)
    mixed = jnp.einsum('gts,bsgd->btgd', matrix, blocks) + mix_bias.T[None, :, :, None]
    gated = (u_act * mixed.reshape(tokens, A)).astype(jnp.bfloat16)
    mix_out = split_sum(gated, out_weight.astype(jnp.bfloat16), N_TP) * out_scale
    middle = (stream + rms_norm(mix_out, gain_mix_out)).astype(jnp.bfloat16)
    ffn_in = rms_norm(middle.astype(jnp.float32), gain_ffn_in).astype(jnp.bfloat16)
    raised = jnp.dot(ffn_in, up_weight.astype(jnp.bfloat16), preferred_element_type=jnp.float32) * up_scale
    hidden = jnp.square(jax.nn.relu(raised)).astype(jnp.bfloat16)
    ffn_out = split_sum(hidden, down_weight.astype(jnp.bfloat16), N_TP) * down_scale
    return (middle.astype(jnp.float32) + rms_norm(ffn_out, gain_ffn_out)).astype(jnp.bfloat16)
```

```python
import functools

import jax
import jax.numpy as jnp
from jax import lax
from jax.experimental import pallas as pl
from jax.experimental.pallas import tpu as pltpu
from jax.sharding import PartitionSpec as P


def fused_kernel(n_out, n_in, *refs):
    resid, v_weight, u_weight, out_weight, up_weight, down_weight = refs[:6]
    gain_mix_in, u_scale, v_scale, v_gain, mix_matrix, mix_bias = refs[6:12]
    out_scale, gain_mix_out, gain_ffn_in, up_scale, down_scale, gain_ffn_out = refs[12:18]
    result = refs[18]
    gathered, acc, x_buf, stream, h_buf, p_recv, f_recv, own_stat, mate_stat, mixers, bias = refs[
        19:30
    ]
    z_send, z_recv, y_send, y_recv, x_send, x_recv, load_sem = refs[30:37]
    t_send, t_recv, c_send, c_recv, out_sem = refs[37:42]
    half, single = jnp.bfloat16, jnp.float32
    parts, members, depth, branch = gathered.shape
    rows, width = acc.shape
    part = width // 2
    pieces = branch // depth
    n_ffn = (parts - 3) // 2
    groups, block = mix_matrix.shape[0], mix_matrix.shape[1]
    chunk = rows // n_out
    member = lax.axis_index("fs")
    rep = lax.axis_index("rep")
    tp = lax.axis_index("tp")
    outer, inner = member // n_in, member % n_in
    peer_in = 1 - inner
    has_left, has_right = outer > 0, outer < n_out - 1
    across, twin, mate = {"fs": outer * n_in + peer_in}, {"rep": 1 - rep}, {"tp": 1 - tp}

    def greet(device):
        pl.semaphore_signal(barrier, inc=1, device_id=device, device_id_type=pl.DeviceIdType.MESH)

    barrier = pltpu.get_barrier_semaphore()
    for step in (1, n_out - 1):
        greet({"fs": lax.rem(outer + step, n_out) * n_in + inner})
    for device in (across, twin, mate):
        greet(device)

    def remote(src, dst, send, recv, device):
        return pltpu.make_async_remote_copy(
            src_ref=src,
            dst_ref=dst,
            send_sem=send,
            recv_sem=recv,
            device_id=device,
            device_id_type=pl.DeviceIdType.MESH,
        )

    def slot(p, index, base, size):
        return gathered.at[p, index, pl.ds(pl.multiple_of(base, depth // 8), size), :]

    def moved(ref, send, recv, device):
        return remote(ref, ref, send, recv, device)

    def z_copy(p, src, right):
        ref = slot(p, src * n_in + inner, rep * (depth // 4), 3 * depth // 4)
        way = right.astype(jnp.int32)
        device = {"fs": (outer + 2 * way - 1) * n_in + inner}
        return moved(ref, z_send.at[p, way, src], z_recv.at[p, src], device)

    def y_copy(p, src):
        ref = slot(p, src * n_in + inner, rep * (depth // 2), depth // 2)
        return moved(ref, y_send.at[p, src], y_recv.at[p, src], across)

    def y_own(p):
        ref = slot(p, member, rep * (depth // 8), 7 * depth // 8)
        return moved(ref, y_send.at[p, outer], y_recv.at[p, outer], across)

    def x_own(p):
        ref = slot(p, outer * n_in + peer_in, rep * (7 * depth // 8), depth // 8)
        return moved(ref, x_send.at[p, outer, 0], x_recv.at[p, outer, 0], twin)

    def x_side(p, src):
        ref = slot(p, src * n_in + inner, rep * (3 * depth // 4), depth // 4)
        return moved(ref, x_send.at[p, src, 0], x_recv.at[p, src, 0], twin)

    def x_diag(p, src):
        ref = slot(p, src * n_in + peer_in, rep * (depth // 2), depth // 2)
        return moved(ref, x_send.at[p, src, 1], x_recv.at[p, src, 1], twin)

    def source(k):
        both = jnp.minimum(outer, n_out - 1 - outer)
        near = k <= 2 * both
        d = jnp.where(near, (k + 1) // 2, k - both)
        long_right = outer < n_out - 1 - outer
        right = jnp.where(near, k % 2 == 0, long_right)
        return jnp.where(right, outer + d, outer - d)

    yes = outer >= 0

    def own_start(p):
        pl.when(has_right)(lambda: z_copy(p, outer, yes).start())
        pl.when(has_left)(lambda: z_copy(p, outer, outer < 0).start())
        y_own(p).start()

    def own_finish(p):
        y_own(p).wait_recv()
        x_own(p).start()

    def onward(src):
        return jnp.where(src < outer, has_right, has_left)

    def first_stage(p, k):
        src = source(k)
        z_copy(p, src, src < outer).wait_recv()
        pl.when(onward(src))(lambda: z_copy(p, src, src < outer).start())
        y_copy(p, src).start()
        x_side(p, src).start()

    def second_stage(p, k):
        src = source(k)
        y_copy(p, src).wait_recv()
        x_diag(p, src).start()

    lag = 2
    others = n_out - 1

    def comm(p, k):
        @pl.when(k == 0)
        def _():
            pl.when(p + 2 < parts)(lambda: own_start(p + 2))
            own_finish(p)

        @pl.when(k > 0)
        def _():
            first_stage(p, k)
            late = p * others + k - 1 - lag
            pl.when(late >= 0)(lambda: second_stage(late // others, late % others + 1))

    def finish(p):
        x_own(p).wait_recv()

        @pl.loop(1, n_out)
        def _(k):
            src = source(k)
            x_side(p, src).wait_recv()
            x_diag(p, src).wait_recv()

    def drain():
        @pl.loop(0, parts)
        def _(p):
            pl.when(has_right)(lambda: z_copy(p, outer, yes).wait_send())
            pl.when(has_left)(lambda: z_copy(p, outer, outer < 0).wait_send())
            y_own(p).wait_send()
            x_own(p).wait_send()

            @pl.loop(1, n_out)
            def _(k):
                src = source(k)
                pl.when(onward(src))(lambda: z_copy(p, src, src < outer).wait_send())
                y_copy(p, src).wait_send()
                x_side(p, src).wait_send()
                x_diag(p, src).wait_send()

    def tile(p):
        return pl.ds((p % n_out) * depth, depth), (p // n_out) * branch

    def loads(p):
        low, left = tile(p)
        if p < 2 or 3 <= p < 3 + n_ffn:
            src = (v_weight, u_weight)[p] if p < 2 else up_weight
            first = 0 if p < 2 else (p - 3) * branch
            return [
                pltpu.make_async_copy(
                    src.at[:, pl.ds(first, branch)],
                    acc.at[low, pl.ds(left, branch)],
                    load_sem.at[p, 0],
                )
            ]
        src, first = (out_weight, 0) if p == 2 else (down_weight, (p - 3 - n_ffn) * branch)
        return [
            pltpu.make_async_copy(
                src.at[pl.ds(first + i * depth, depth), :],
                acc.at[low, pl.ds(left + i * depth, depth)],
                load_sem.at[p, i],
            )
            for i in range(pieces)
        ]

    def cast(p):
        for copy in loads(p):
            copy.wait()
        low, left = tile(p)
        if p < 2 or 3 <= p < 3 + n_ffn:
            gathered[p, member] = acc[low, pl.ds(left, branch)].astype(half)
            return
        scale = (out_scale if p == 2 else down_scale)[...]
        for i in range(pieces):
            values = acc[low, pl.ds(left + i * depth, depth)] * scale
            gathered[p, member, :, pl.ds(i * depth, depth)] = values.astype(half)

    for p in (0, 1):
        for copy in loads(p):
            copy.start()
    fetch = pltpu.make_async_copy(resid, stream.at[tp], out_sem.at[0])
    fetch.start()
    for p in range(2, parts):
        for copy in loads(p):
            copy.start()
    cast(0)
    cast(1)
    swap = remote(stream.at[tp], stream.at[tp], t_send.at[0], t_recv.at[0], mate)
    pl.semaphore_wait(barrier, 5)
    own_start(0)
    own_start(1)
    fetch.wait()
    swap.start()
    for p in range(2, parts):
        cast(p)
    mixers[...] = mix_matrix[...].reshape(groups * block, block).astype(half)
    span = branch // groups
    turned = mix_bias[...].T
    lanes = lax.broadcasted_iota(jnp.int32, (block, 128), 1)
    for first in range(0, branch, 128):
        column = turned[:, first // span : first // span + 1]
        level = jnp.broadcast_to(column, (block, 128))
        for g in range(first // span + 1, (first + 127) // span + 1):
            level = jnp.where(lanes >= g * span - first, turned[:, g : g + 1], level)
        bias[:, pl.ds(first, 128)] = level
    swap.wait()

    def here(k):
        return pl.ds(pl.multiple_of(k * chunk, chunk), chunk)

    def dot(a, b):
        return jnp.dot(a, b, preferred_element_type=single)

    def spanned(p):
        return gathered[p].reshape(width, branch)

    def norm_stage(k):
        r = here(k)
        a, b = stream[0, r, :].astype(single), stream[1, r, :].astype(single)
        power = jnp.sum(a * a, axis=1, keepdims=True) + jnp.sum(b * b, axis=1, keepdims=True)
        scale = lax.rsqrt(power / width + 1e-06)
        x_buf[r, pl.ds(0, part)] = (a * scale * gain_mix_in[:, :part]).astype(half)
        x_buf[r, pl.ds(part, part)] = (b * scale * gain_mix_in[:, part:]).astype(half)

    def v_stage(k):
        r = here(k)
        act = jax.nn.gelu(dot(x_buf[r, :], spanned(0)) * v_scale[...])
        acc[r, pl.ds(0, branch)] = act
        total = jnp.sum(act, axis=1, keepdims=True)
        squares = jnp.sum(act * act, axis=1, keepdims=True)
        lane = lax.broadcasted_iota(jnp.int32, (chunk, 128), 1)
        own_stat[r, :] = jnp.where(lane == 0, total, squares)

    stat_copy = remote(own_stat, mate_stat.at[0], t_send.at[1], t_recv.at[1], mate)

    def u_stage(k):
        pl.when(k == 0)(lambda: stat_copy.start())
        r = here(k)
        act = jax.nn.gelu(dot(x_buf[r, :], spanned(1)) * u_scale[...])
        acc[r, pl.ds(branch, branch)] = act

    def p_copy(k):
        r = here(k)
        return remote(h_buf.at[r, :], p_recv.at[r, :], c_send.at[k, 0], c_recv.at[k, 0], mate)

    def times(values, p, m):
        total = dot(values[:, :depth], gathered[p, m, :, pl.ds(0, depth)])
        for i in range(1, pieces):
            total += dot(
                values[:, i * depth : (i + 1) * depth], gathered[p, m, :, pl.ds(i * depth, depth)]
            )
        return total

    def out_stage(k):
        pl.when(k == 0)(lambda: stat_copy.wait())
        pl.when(k > 0)(lambda: p_copy(k - 1).start())
        r = here(k)
        sums = own_stat[r, :] + mate_stat[0, r, :]
        centre = sums[:, 0:1] / (2 * branch)
        spread = sums[:, 1:2] / (2 * branch) - centre * centre
        scale = lax.rsqrt(spread + 1e-06)
        normed = ((acc[r, pl.ds(0, branch)] - centre) * scale * v_gain[...]).astype(half)
        per = 256 // span
        lane = lax.broadcasted_iota(jnp.int32, (block, 256), 1)
        gates = []
        for b in range(chunk // block):
            line = []
            for q in range(branch // 256):
                both = dot(
                    mixers[pl.ds(q * per * block, per * block), :],
                    normed[b * block : (b + 1) * block, q * 256 : (q + 1) * 256],
                )
                mixed = both[:block]
                for g in range(1, per):
                    mixed = jnp.where(lane >= g * span, both[g * block : (g + 1) * block], mixed)
                line.append(mixed + bias[:, pl.ds(q * 256, 256)])
            gates.append(jnp.concatenate(line, axis=1))
        gate = jnp.concatenate(gates, axis=0)
        gated = (acc[r, pl.ds(branch, branch)] * gate).astype(half)
        for m in range(members):
            h_buf[r, pl.ds(m * depth, depth)] = times(gated, 2, m).astype(half)

    def mid_stage(k):
        pl.when(k == 0)(lambda: p_copy(n_out - 1).start())
        p_copy(k).wait()
        r = here(k)
        mix = h_buf[r, :].astype(single) + p_recv[r, :].astype(single)
        scale = lax.rsqrt(jnp.sum(mix * mix, axis=1, keepdims=True) / width + 1e-06)
        mix = mix * scale * gain_mix_out[...]
        a = (stream[0, r, :].astype(single) + mix[:, :part]).astype(half)
        b = (stream[1, r, :].astype(single) + mix[:, part:]).astype(half)
        stream[0, r, :] = a
        stream[1, r, :] = b
        a, b = a.astype(single), b.astype(single)
        power = jnp.sum(a * a, axis=1, keepdims=True) + jnp.sum(b * b, axis=1, keepdims=True)
        scale = lax.rsqrt(power / width + 1e-06)
        x_buf[r, pl.ds(0, part)] = (a * scale * gain_ffn_in[:, :part]).astype(half)
        x_buf[r, pl.ds(part, part)] = (b * scale * gain_ffn_in[:, part:]).astype(half)

    def strip(j):
        return pl.ds(pl.multiple_of(j * branch, branch), branch)

    def up_stage(k, p):
        r, cols = here(k), strip(p - 3)
        raised = jax.nn.relu(dot(x_buf[r, :], spanned(p)) * up_scale[:, cols])
        h_buf[r, cols] = (raised * raised).astype(half)

    def down_stage(k, p, fresh):
        r = here(k)
        values = h_buf[r, strip(p - 3 - n_ffn)]
        for m in range(members):
            cols = pl.ds(m * depth, depth)
            terms = times(values, p, m)
            acc[r, cols] = terms if fresh else acc[r, cols] + terms

    def segment(p, needs, *stages):
        @pl.loop(0, n_out)
        def _(k):
            comm(p, k)
            if needs is not None:
                pl.when(k == 0)(lambda: finish(needs))
            for stage in stages:
                stage(k)

    segment(0, None)
    segment(1, None, norm_stage)
    segment(2, 0, v_stage)
    segment(3, 1, u_stage)
    segment(4, 2, out_stage)
    segment(5, 3, mid_stage, lambda k: up_stage(k, 3))

    @pl.loop(6, 5 + n_ffn)
    def _(p):
        segment(p, p - 2, lambda k: up_stage(k, p - 2))

    for p in range(5 + n_ffn, parts):
        segment(p, p - 2, lambda k: down_stage(k, p - 2, p == 5 + n_ffn))
    last = parts - 1
    for late in range(parts * others - lag, parts * others):
        second_stage(late // others, late % others + 1)

    finish(last - 1)

    @pl.loop(0, n_out)
    def _(k):
        down_stage(k, last - 1, False)

    finish(last)
    share = members // 2

    def f_copy(k):
        r = here(k)
        return remote(
            x_buf.at[r, pl.ds(0, part)], f_recv.at[r, :], c_send.at[k, 1], c_recv.at[k, 1], mate
        )

    def s_copy(k):
        r = here(k)
        return remote(
            own_stat.at[r, :], mate_stat.at[1, r, :], c_send.at[k, 0], c_recv.at[k, 0], mate
        )

    def own_cols(m):
        return pl.ds(pl.multiple_of(m * depth, depth), depth)

    @pl.loop(0, n_out)
    def _(k):
        r = here(k)
        values = h_buf[r, pl.ds((n_ffn - 1) * branch, branch)]
        for i in range(share):
            m = (1 - tp) * share + i
            terms = acc[r, own_cols(m)] + times(values, last, m)
            x_buf[r, pl.ds(i * depth, depth)] = terms.astype(half)
        pl.when(k > 0)(lambda: f_copy(k - 1).start())

    f_copy(n_out - 1).start()

    @pl.loop(0, n_out)
    def _(k):
        r = here(k)
        values = h_buf[r, pl.ds((n_ffn - 1) * branch, branch)]
        kept = []
        for i in range(share):
            m = tp * share + i
            terms = acc[r, own_cols(m)] + times(values, last, m)
            kept.append(terms.astype(half).astype(single))
        f_copy(k).wait()
        power = jnp.zeros((chunk, 1), single)
        for i in range(share):
            total = kept[i] + f_recv[r, pl.ds(i * depth, depth)].astype(single)
            power += jnp.sum(total * total, axis=1, keepdims=True)
            acc[r, own_cols(tp * share + i)] = total
        own_stat[r, :] = jnp.broadcast_to(power, (chunk, 128))
        pl.when(k > 0)(lambda: s_copy(k - 1).start())

    s_copy(n_out - 1).start()
    drain()

    def leave(k):
        r = here(k)
        return pltpu.make_async_copy(
            x_buf.at[r, pl.ds(part, part)], result.at[r, :], out_sem.at[k]
        )

    @pl.loop(0, n_out)
    def _(k):
        s_copy(k).wait()
        r = here(k)
        power = own_stat[r, 0:1] + mate_stat[1, r, 0:1]
        scale = lax.rsqrt(power / width + 1e-06)
        cols = pl.ds(pl.multiple_of(tp * part, part), part)
        total = acc[r, cols] * scale * gain_ffn_out[:, cols]
        x_buf[r, pl.ds(part, part)] = (stream[tp, r, :].astype(single) + total).astype(half)
        leave(k).start()

    for k in range(n_out):
        leave(k).wait()


def rms_norm(values, gain, width, power_sum):
    return values * lax.rsqrt(power_sum / width + 1e-06) * gain


def local(
    resid,
    gain_mix_in,
    u_weight,
    v_weight,
    u_scale,
    v_scale,
    v_gain,
    mix_matrix,
    mix_bias,
    out_weight,
    out_scale,
    gain_mix_out,
    gain_ffn_in,
    up_weight,
    up_scale,
    down_weight,
    down_scale,
    gain_ffn_out,
):
    rows = resid.shape[0]
    part_width = resid.shape[1]
    width = part_width * lax.axis_size("tp")
    lane = lax.axis_index("tp")
    full_rows = lax.all_gather(resid, "tp", axis=1, tiled=True)
    out_scales, down_scales = (
        lax.all_gather(out_scale, "fs", axis=0, tiled=True),
        lax.all_gather(down_scale, "fs", axis=0, tiled=True),
    )
    full_float = full_rows.astype(jnp.float32)
    normed = rms_norm(
        full_float, gain_mix_in, width, jnp.sum(full_float * full_float, axis=1, keepdims=True)
    ).astype(jnp.bfloat16)
    branch_cols = u_weight.shape[1]
    u_pre = jnp.dot(
        normed,
        lax.all_gather(u_weight.astype(jnp.bfloat16), "fs", axis=0, tiled=True),
        preferred_element_type=jnp.float32,
    )
    v_pre = jnp.dot(
        normed,
        lax.all_gather(v_weight.astype(jnp.bfloat16), "fs", axis=0, tiled=True),
        preferred_element_type=jnp.float32,
    )
    u_act = jax.nn.gelu(u_pre * u_scale)
    v_act = jax.nn.gelu(v_pre * v_scale)
    total, squares = lax.psum(
        (jnp.sum(v_act, axis=1, keepdims=True), jnp.sum(v_act * v_act, axis=1, keepdims=True)), "tp"
    )
    branch_width = branch_cols * lax.axis_size("tp")
    centre = total / branch_width
    spread = squares / branch_width - centre * centre
    v_norm = ((v_act - centre) * lax.rsqrt(spread + 1e-06) * v_gain).astype(jnp.bfloat16)
    groups = mix_matrix.shape[0]
    block = mix_matrix.shape[1]
    blocks = v_norm.reshape(rows // block, block, groups, branch_cols // groups)
    mixed = (
        jnp.einsum(
            "gts,bsgd->btgd",
            mix_matrix.astype(jnp.bfloat16),
            blocks,
            preferred_element_type=jnp.float32,
        )
        + mix_bias.T[None, :, :, None]
    )
    gated = (u_act * mixed.reshape(rows, branch_cols)).astype(jnp.bfloat16)
    partial_value = jnp.dot(
        gated,
        lax.all_gather(out_weight.astype(jnp.bfloat16), "fs", axis=1, tiled=True),
        preferred_element_type=jnp.float32,
    )
    mix_out = lax.psum(partial_value.astype(jnp.bfloat16), "tp").astype(jnp.float32) * out_scales
    power = jnp.sum(mix_out * mix_out, axis=1, keepdims=True)
    middle_full = (full_float + rms_norm(mix_out, gain_mix_out, width, power)).astype(jnp.bfloat16)
    middle = lax.dynamic_slice_in_dim(middle_full, lane * part_width, part_width, 1)
    middle_float = middle_full.astype(jnp.float32)
    ffn_in = rms_norm(
        middle_float,
        gain_ffn_in,
        width,
        jnp.sum(middle_float * middle_float, axis=1, keepdims=True),
    ).astype(jnp.bfloat16)
    up_half = up_weight.astype(jnp.bfloat16)
    down_half = down_weight.astype(jnp.bfloat16)
    whole_up = lax.all_gather(up_half, "fs", axis=0, tiled=True)
    raised = jnp.dot(ffn_in, whole_up, preferred_element_type=jnp.float32)
    hidden = jnp.square(jax.nn.relu(raised * up_scale)).astype(jnp.bfloat16)
    whole_down = lax.all_gather(down_half, "fs", axis=1, tiled=True)
    terms = jnp.dot(hidden, whole_down, preferred_element_type=jnp.float32)
    own_down = lax.dynamic_slice_in_dim(down_scales, lane * part_width, part_width, 0)
    ffn_out = (
        lax.psum_scatter(terms.astype(jnp.bfloat16), "tp", scatter_dimension=1, tiled=True).astype(
            jnp.float32
        )
        * own_down
    )
    power_out = lax.psum(jnp.sum(ffn_out * ffn_out, axis=1, keepdims=True), "tp")
    own_gain_out = lax.dynamic_slice_in_dim(gain_ffn_out, lane * part_width, part_width, 0)
    return (middle.astype(jnp.float32) + rms_norm(ffn_out, own_gain_out, width, power_out)).astype(
        jnp.bfloat16
    )


def local_fast(
    resid,
    gain_mix_in,
    u_weight,
    v_weight,
    u_scale,
    v_scale,
    v_gain,
    mix_matrix,
    mix_bias,
    out_weight,
    out_scale,
    gain_mix_out,
    gain_ffn_in,
    up_weight,
    up_scale,
    down_weight,
    down_scale,
    gain_ffn_out,
):
    rows, part = resid.shape
    members = lax.axis_size("fs")
    width = part * 2
    depth, branch = v_weight.shape
    hidden = up_weight.shape[1]
    parts = 3 + 2 * (hidden // branch)
    n_in = 2
    n_out = members // n_in
    half, single = jnp.bfloat16, jnp.float32
    groups, block = mix_matrix.shape[0], mix_matrix.shape[1]

    def row(vector):
        return vector.reshape(1, -1)

    big = [resid, v_weight, u_weight, out_weight, up_weight, down_weight]
    small = [
        row(gain_mix_in),
        row(u_scale),
        row(v_scale),
        row(v_gain),
        mix_matrix,
        mix_bias,
        row(out_scale),
        row(gain_mix_out),
        row(gain_ffn_in),
        row(up_scale),
        row(down_scale),
        row(gain_ffn_out),
    ]
    dma = pltpu.SemaphoreType.DMA
    scratch = [
        pltpu.VMEM((parts, members, depth, branch), half),
        pltpu.VMEM((rows, width), single),
        pltpu.VMEM((rows, width), half),
        pltpu.VMEM((2, rows, part), half),
        pltpu.VMEM((rows, width), half),
        pltpu.VMEM((rows, width), half),
        pltpu.VMEM((rows, part), half),
        pltpu.VMEM((rows, 128), single),
        pltpu.VMEM((2, rows, 128), single),
        pltpu.VMEM((groups * block, block), half),
        pltpu.VMEM((block, branch), single),
        dma((parts, 2, n_out)),
        dma((parts, n_out)),
        dma((parts, n_out)),
        dma((parts, n_out)),
        dma((parts, n_out, 2)),
        dma((parts, n_out, 2)),
        dma((parts, branch // depth)),
        dma((2,)),
        dma((2,)),
        dma((n_out, 2)),
        dma((n_out, 2)),
        dma((n_out,)),
    ]
    return pl.pallas_call(
        functools.partial(fused_kernel, n_out, n_in),
        out_shape=jax.ShapeDtypeStruct((rows, part), half),
        in_specs=[pl.BlockSpec(memory_space=pl.ANY)] * len(big)
        + [pl.BlockSpec(memory_space=pltpu.VMEM)] * len(small),
        out_specs=pl.BlockSpec(memory_space=pl.ANY),
        scratch_shapes=scratch,
        compiler_params=pltpu.CompilerParams(
            collective_id=0, has_side_effects=True, vmem_limit_bytes=63 * 1024 * 1024
        ),
        name="fused_layer",
    )(*big, *small)


def solution(mesh):
    in_specs = (
        P(("rep", "fs"), "tp"),
        P(),
        P("fs", "tp"),
        P("fs", "tp"),
        P("tp"),
        P("tp"),
        P("tp"),
        P("tp", None, None),
        P("tp", None),
        P("tp", "fs"),
        P("fs"),
        P(),
        P(),
        P("fs", "tp"),
        P("tp"),
        P("tp", "fs"),
        P("fs"),
        P(),
    )
    out_specs = P(("rep", "fs"), "tp")
    sizes = mesh.shape

    def whole(*args):
        rows = args[0].shape[0] // (sizes["rep"] * sizes["fs"])
        width = args[0].shape[1]
        branch = args[2].shape[1] // sizes["tp"]
        hidden = args[13].shape[1] // sizes["tp"]
        groups, block = args[7].shape[0] // sizes["tp"], args[7].shape[1]
        planes, depth = sizes["fs"] // 2, width // sizes["fs"]
        paired = sizes["rep"] == 2 and sizes["tp"] == 2 and sizes["fs"] % 4 == 0
        fits = depth % 256 == 0 and branch % depth == 0 and hidden % branch == 0
        blocks = rows % (planes * block) == 0 and (256 * groups) % branch == 0
        small = 2 * width * (3 * branch + 2 * hidden) <= 24 * 1024 * 1024
        fast = paired and planes >= 2 and fits and blocks and small
        return mapped(local_fast if fast else local)(*args)

    def mapped(body):
        return jax.shard_map(
            body, mesh=mesh, in_specs=in_specs, out_specs=out_specs, check_vma=False
        )

    return whole
```

```python
import functools

import jax
import jax.numpy as jnp
from jax import lax
from jax.experimental import pallas as pl
from jax.experimental.pallas import tpu as pltpu
from jax.sharding import PartitionSpec as P


def fused_kernel(n_out, n_in, *refs):
    resid, v_weight, u_weight, out_weight, up_weight, down_weight = refs[:6]
    gain_mix_in, u_scale, v_scale, v_gain, mix_matrix, mix_bias = refs[6:12]
    out_scale, gain_mix_out, gain_ffn_in, up_scale, down_scale, gain_ffn_out = refs[12:18]
    result = refs[18]
    gathered, acc, x_buf, x_twin, stream, h_buf, terms, p_recv, d_recv, o_recv = refs[19:29]
    own_stat, mate_stat, mixers, bias = refs[29:33]
    z_send, z_recv, e_send, e_recv, y_send, y_recv, x_send, x_recv, load_sem = refs[33:42]
    t_send, t_recv, c_send, c_recv, a_send, a_recv, d_send, d_sem, o_send, o_sem, out_sem = refs[
        42:53
    ]
    half, single = jnp.bfloat16, jnp.float32
    parts, members, depth, branch = gathered.shape
    rows, width = x_buf.shape
    part = width // 2
    shared = h_buf.shape[2]
    pieces = branch // depth
    n_ffn = (parts - 3) // 2
    groups, block = mix_matrix.shape[0], mix_matrix.shape[1]
    chunk = rows // n_out
    member = lax.axis_index("fs")
    rep = lax.axis_index("rep")
    tp = lax.axis_index("tp")
    outer, inner = member // n_in, member % n_in
    peer_in = 1 - inner
    cut = 3 * depth // 16
    has_left, has_right = outer > 0, outer < n_out - 1
    across, twin, mate = {"fs": outer * n_in + peer_in}, {"rep": 1 - rep}, {"tp": 1 - tp}

    def greet(device):
        pl.semaphore_signal(barrier, inc=1, device_id=device, device_id_type=pl.DeviceIdType.MESH)

    barrier = pltpu.get_barrier_semaphore()
    for step in (1, n_out - 1):
        greet({"fs": lax.rem(outer + step, n_out) * n_in + inner})
    for device in (across, twin, mate):
        greet(device)

    def remote(src, dst, send, recv, device):
        return pltpu.make_async_remote_copy(
            src_ref=src,
            dst_ref=dst,
            send_sem=send,
            recv_sem=recv,
            device_id=device,
            device_id_type=pl.DeviceIdType.MESH,
        )

    def slot(p, index, base, size):
        return gathered.at[p, index, pl.ds(pl.multiple_of(base, depth // 16), size), :]

    def moved(ref, send, recv, device):
        return remote(ref, ref, send, recv, device)

    def z_copy(p, src, right):
        whole = p >= 3
        base, size = (0, depth) if whole else (rep * (depth // 4), 3 * depth // 4)
        ref = slot(p, src * n_in + inner, base, size)
        way = right.astype(jnp.int32)
        device = {"fs": (outer + 2 * way - 1) * n_in + inner}
        return moved(ref, z_send.at[p, way, src], z_recv.at[p, src], device)

    def e_copy(p, src, right):
        ref = slot(p, src * n_in + peer_in, 0, cut)
        way = right.astype(jnp.int32)
        device = {"fs": (outer + 2 * way - 1) * n_in + inner}
        return moved(ref, e_send.at[p - 3, way, src], e_recv.at[p - 3, src], device)

    def y_copy(p, src):
        base, size = (cut, depth - cut) if p >= 3 else (rep * (depth // 2), depth // 2)
        ref = slot(p, src * n_in + inner, base, size)
        return moved(ref, y_send.at[p, src], y_recv.at[p, src], across)

    def y_own(p):
        base, size = (0, depth) if p >= 3 else (rep * (depth // 8), 7 * depth // 8)
        ref = slot(p, member, base, size)
        return moved(ref, y_send.at[p, outer], y_recv.at[p, outer], across)

    def x_own(p):
        ref = slot(p, outer * n_in + peer_in, rep * (7 * depth // 8), depth // 8)
        return moved(ref, x_send.at[p, outer, 0], x_recv.at[p, outer, 0], twin)

    def x_side(p, src):
        ref = slot(p, src * n_in + inner, rep * (3 * depth // 4), depth // 4)
        return moved(ref, x_send.at[p, src, 0], x_recv.at[p, src, 0], twin)

    def x_diag(p, src):
        ref = slot(p, src * n_in + peer_in, rep * (depth // 2), depth // 2)
        return moved(ref, x_send.at[p, src, 1], x_recv.at[p, src, 1], twin)

    def source(k):
        both = jnp.minimum(outer, n_out - 1 - outer)
        near = k <= 2 * both
        d = jnp.where(near, (k + 1) // 2, k - both)
        long_right = outer < n_out - 1 - outer
        right = jnp.where(near, k % 2 == 0, long_right)
        return jnp.where(right, outer + d, outer - d)

    yes = outer >= 0

    def own_start(p):
        both_ways(z_copy, p, begin)
        y_own(p).start()

    def both_ways(copy, p, act):
        pl.when(has_right)(lambda: act(copy(p, outer, yes)))
        pl.when(has_left)(lambda: act(copy(p, outer, outer < 0)))

    def begin(copy):
        copy.start()

    def own_finish(p):
        y_own(p).wait_recv()
        if p < 3:
            x_own(p).start()
        else:
            both_ways(e_copy, p, begin)

    def onward(src):
        return jnp.where(src < outer, has_right, has_left)

    def first_stage(p, k):
        src = source(k)
        z_copy(p, src, src < outer).wait_recv()
        pl.when(onward(src))(lambda: z_copy(p, src, src < outer).start())
        y_copy(p, src).start()
        if p < 3:
            x_side(p, src).start()

    def second_stage(p, k):
        src = source(k)
        if p < 3:
            y_copy(p, src).wait_recv()
            x_diag(p, src).start()
        else:
            e_copy(p, src, src < outer).wait_recv()
            pl.when(onward(src))(lambda: e_copy(p, src, src < outer).start())

    others = n_out - 1

    def comm(p, k):
        @pl.when(k == 0)
        def _():
            own_finish(p)
            if p > 0:
                second_stage(p - 1, others)

        @pl.when(k > 0)
        def _():
            first_stage(p, k)
            pl.when(k > 1)(lambda: second_stage(p, k - 1))

    def finish(p):
        if p < 3:
            x_own(p).wait_recv()

        @pl.loop(1, n_out)
        def _(k):
            src = source(k)
            if p < 3:
                x_side(p, src).wait_recv()
                x_diag(p, src).wait_recv()
            else:
                y_copy(p, src).wait_recv()

    def settle(copy):
        copy.wait_send()

    def drain():
        for p in range(parts):
            both_ways(z_copy, p, settle)
            y_own(p).wait_send()
            if p < 3:
                x_own(p).wait_send()
            else:
                both_ways(e_copy, p, settle)

            @pl.loop(1, n_out)
            def _(k):
                src = source(k)
                pl.when(onward(src))(lambda: z_copy(p, src, src < outer).wait_send())
                y_copy(p, src).wait_send()
                if p < 3:
                    x_side(p, src).wait_send()
                    x_diag(p, src).wait_send()
                else:
                    pl.when(onward(src))(lambda: e_copy(p, src, src < outer).wait_send())

    def tile(p):
        return pl.ds((p % n_out) * depth, depth), (p // n_out) * branch

    def loads(p):
        low, left = tile(p)
        if p < 2 or 3 <= p < 3 + n_ffn:
            src = (v_weight, u_weight)[p] if p < 2 else up_weight
            first = 0 if p < 2 else rep * shared + (p - 3) * branch
            return [
                pltpu.make_async_copy(
                    src.at[:, pl.ds(first if p < 2 else pl.multiple_of(first, branch), branch)],
                    acc.at[low, pl.ds(left, branch)],
                    load_sem.at[p, 0],
                )
            ]
        src, first = (out_weight, outer * 0) if p == 2 else (down_weight, rep * shared + (p - 3 - n_ffn) * branch)
        return [
            pltpu.make_async_copy(
                src.at[pl.ds(pl.multiple_of(first + i * depth, depth), depth), :],
                acc.at[low, pl.ds(left + i * depth, depth)],
                load_sem.at[p, i],
            )
            for i in range(pieces)
        ]

    def cast(p):
        for copy in loads(p):
            copy.wait()
        low, left = tile(p)
        if p < 2 or 3 <= p < 3 + n_ffn:
            gathered[p, member] = acc[low, pl.ds(left, branch)].astype(half)
            return
        scale = (out_scale if p == 2 else down_scale)[...]
        for i in range(pieces):
            values = acc[low, pl.ds(left + i * depth, depth)] * scale
            gathered[p, member, :, pl.ds(i * depth, depth)] = values.astype(half)

    for p in (0, 1):
        for copy in loads(p):
            copy.start()
    fetch = pltpu.make_async_copy(resid, stream.at[tp], out_sem.at[0])
    fetch.start()
    for p in range(2, parts):
        for copy in loads(p):
            copy.start()
    cast(0)
    cast(1)
    swap = remote(stream.at[tp], stream.at[tp], t_send.at[0], t_recv.at[0], mate)
    pl.semaphore_wait(barrier, 5)
    own_start(0)
    own_start(1)
    fetch.wait()
    swap.start()
    for p in range(2, parts):
        cast(p)
    mixers[...] = mix_matrix[...].reshape(groups * block, block).astype(half)
    span = branch // groups
    turned = mix_bias[...].T
    lanes = lax.broadcasted_iota(jnp.int32, (block, 128), 1)
    for first in range(0, branch, 128):
        column = turned[:, first // span : first // span + 1]
        level = jnp.broadcast_to(column, (block, 128))
        for g in range(first // span + 1, (first + 127) // span + 1):
            level = jnp.where(lanes >= g * span - first, turned[:, g : g + 1], level)
        bias[:, pl.ds(first, 128)] = level
    swap.wait()

    def here(k):
        return pl.ds(pl.multiple_of(k * chunk, chunk), chunk)

    def dot(a, b):
        return jnp.dot(a, b, preferred_element_type=single)

    def spanned(p):
        return gathered[p].reshape(width, branch)

    def norm_stage(k):
        r = here(k)
        a, b = stream[0, r, :].astype(single), stream[1, r, :].astype(single)
        power = jnp.sum(a * a, axis=1, keepdims=True) + jnp.sum(b * b, axis=1, keepdims=True)
        scale = lax.rsqrt(power / width + 1e-06)
        x_buf[r, pl.ds(0, part)] = (a * scale * gain_mix_in[:, :part]).astype(half)
        x_buf[r, pl.ds(part, part)] = (b * scale * gain_mix_in[:, part:]).astype(half)

    def v_stage(k):
        r = here(k)
        act = jax.nn.gelu(dot(x_buf[r, :], spanned(0)) * v_scale[...])
        acc[r, pl.ds(0, branch)] = act
        total = jnp.sum(act, axis=1, keepdims=True)
        squares = jnp.sum(act * act, axis=1, keepdims=True)
        lane = lax.broadcasted_iota(jnp.int32, (chunk, 128), 1)
        own_stat[r, :] = jnp.where(lane == 0, total, squares)

    stat_copy = remote(own_stat, mate_stat.at[0], t_send.at[1], t_recv.at[1], mate)

    def u_stage(k):
        pl.when(k == 0)(lambda: stat_copy.start())
        r = here(k)
        act = jax.nn.gelu(dot(x_buf[r, :], spanned(1)) * u_scale[...])
        acc[r, pl.ds(branch, branch)] = act

    def p_copy(k):
        r = here(k)
        return remote(terms.at[0, r, :], p_recv.at[r, :], c_send.at[k, 0], c_recv.at[k, 0], mate)

    def times(values, p, m):
        total = dot(values[:, :depth], gathered[p, m, :, pl.ds(0, depth)])
        for i in range(1, pieces):
            total += dot(
                values[:, i * depth : (i + 1) * depth], gathered[p, m, :, pl.ds(i * depth, depth)]
            )
        return total

    def out_stage(k):
        r = here(k)
        sums = own_stat[r, :] + mate_stat[0, r, :]
        centre = sums[:, 0:1] / (2 * branch)
        spread = sums[:, 1:2] / (2 * branch) - centre * centre
        scale = lax.rsqrt(spread + 1e-06)
        normed = ((acc[r, pl.ds(0, branch)] - centre) * scale * v_gain[...]).astype(half)
        per = 256 // span
        lane = lax.broadcasted_iota(jnp.int32, (block, 256), 1)
        gates = []
        for b in range(chunk // block):
            line = []
            for q in range(branch // 256):
                both = dot(
                    mixers[pl.ds(q * per * block, per * block), :],
                    normed[b * block : (b + 1) * block, q * 256 : (q + 1) * 256],
                )
                mixed = both[:block]
                for g in range(1, per):
                    mixed = jnp.where(lane >= g * span, both[g * block : (g + 1) * block], mixed)
                line.append(mixed + bias[:, pl.ds(q * 256, 256)])
            gates.append(jnp.concatenate(line, axis=1))
        gate = jnp.concatenate(gates, axis=0)
        gated = (acc[r, pl.ds(branch, branch)] * gate).astype(half)
        for m in range(members):
            terms[0, r, pl.ds(m * depth, depth)] = times(gated, 2, m).astype(half)

    def mid_stage(k):
        p_copy(k).wait()
        r = here(k)
        mix = terms[0, r, :].astype(single) + p_recv[r, :].astype(single)
        scale = lax.rsqrt(jnp.sum(mix * mix, axis=1, keepdims=True) / width + 1e-06)
        mix = mix * scale * gain_mix_out[...]
        a = (stream[0, r, :].astype(single) + mix[:, :part]).astype(half)
        b = (stream[1, r, :].astype(single) + mix[:, part:]).astype(half)
        stream[0, r, :] = a
        stream[1, r, :] = b
        a, b = a.astype(single), b.astype(single)
        power = jnp.sum(a * a, axis=1, keepdims=True) + jnp.sum(b * b, axis=1, keepdims=True)
        scale = lax.rsqrt(power / width + 1e-06)
        x_buf[r, pl.ds(0, part)] = (a * scale * gain_ffn_in[:, :part]).astype(half)
        x_buf[r, pl.ds(part, part)] = (b * scale * gain_ffn_in[:, part:]).astype(half)

    half_cols = pl.ds(pl.multiple_of(tp * part, part), part)

    def a_copy(k):
        r = here(k)
        return remote(
            x_buf.at[r, half_cols], x_twin.at[r, half_cols], a_send.at[k, 0], a_recv.at[k, 0], twin
        )

    def b_copy(k):
        r = here(k)
        return remote(
            x_twin.at[r, half_cols], x_twin.at[r, half_cols], a_send.at[k, 1], a_recv.at[k, 1], mate
        )

    def pass_on(k):
        a_copy(k).wait_recv()
        b_copy(k).start()

    def up_stage(w, k, j):
        r = here(k)
        source_rows = x_twin if w else x_buf
        scale = up_scale[:, pl.ds(pl.multiple_of(rep * shared + j * branch, branch), branch)]
        raised = jax.nn.relu(dot(source_rows[r, :], spanned(3 + j)) * scale)
        h_buf[w, r, pl.ds(j * branch, branch)] = (raised * raised).astype(half)

    planes = n_out // 2
    block_cols = n_in * depth

    def wide(src):
        return pl.ds(pl.multiple_of(src * block_cols, block_cols), block_cols)

    def narrow(src):
        return wide(src % planes)

    def d_copy(src, q):
        w, r = (0, pl.ds(0, rows)) if q is None else (1, pl.ds(q * (rows // 2), rows // 2))
        lane = 0 if q is None else 1 + q
        return remote(
            terms.at[w, r, wide(src)],
            d_recv.at[w, r, narrow(src)],
            d_send.at[lane, src],
            d_sem.at[lane, src],
            mate,
        )

    def o_copy(src, q):
        r = pl.ds(q * (rows // 2), rows // 2)
        return remote(
            terms.at[1, r, wide(src)],
            o_recv.at[r, narrow(src)],
            o_send.at[src, q],
            o_sem.at[src, q],
            twin,
        )

    def mine(src):
        return src // planes == tp

    def down(k, q):
        src = source(k)
        w, low, high = (0, 0, n_out) if q is None else (1, q * planes, (q + 1) * planes)

        @pl.loop(low, high)
        def _(c):
            r = here(c)
            values = h_buf[w, r, :]
            for i in range(n_in):
                m = src * n_in + i
                total = times(values[:, :branch], 3 + n_ffn, m)
                for j in range(1, n_ffn):
                    total += times(values[:, j * branch : (j + 1) * branch], 3 + n_ffn + j, m)
                cols = pl.ds(pl.multiple_of(m * depth, depth), depth)
                terms[w, r, cols] = total.astype(half)

        pl.when(jnp.logical_not(mine(src)))(lambda: d_copy(src, q).start())

    def merge(k, q):
        src = source(k)

        @pl.when(mine(src))
        def _():
            d_copy(src, q).wait_recv()

            @pl.loop(q * planes, (q + 1) * planes)
            def _(c):
                r = here(c)
                total = terms[1, r, wide(src)].astype(single)
                total += d_recv[1, r, narrow(src)].astype(single)
                terms[1, r, wide(src)] = total.astype(half)

            o_copy(src, q).start()

    def gather_group(k):
        src = source(k)

        @pl.when(mine(src))
        def _():
            d_copy(src, None).wait_recv()
            o_copy(src, 0).wait_recv()
            o_copy(src, 1).wait_recv()

            @pl.loop(0, n_out)
            def _(c):
                r = here(c)
                total = terms[0, r, wide(src)].astype(single)
                total += d_recv[0, r, narrow(src)].astype(single)
                total += o_recv[r, narrow(src)].astype(single)
                acc[r, narrow(src)] = total
                power = jnp.sum(total * total, axis=1, keepdims=True)
                own_stat[r, :] += jnp.broadcast_to(power, (chunk, 128))

    def segment(p, *stages):
        @pl.loop(0, n_out)
        def _(k):
            comm(p, k)
            for stage in stages:
                stage(k)

    def each(stage):
        pl.loop(0, n_out)(stage)

    up_parts = range(3, 3 + n_ffn)
    down_parts = range(3 + n_ffn, parts)
    final = n_out - 1
    middle = jnp.logical_and(has_left, has_right)

    def nearest(stage, p):
        stage(p, 1)
        pl.when(middle)(lambda: stage(p, 2))

    def second(stage, p):
        stage(p, jnp.where(middle, 3, 2))

    def third(stage, p):
        pl.when(jnp.logical_not(middle))(lambda: stage(p, 3))

    segment(0)
    own_start(2)
    segment(1, norm_stage)
    finish(0)
    segment(2, v_stage)
    own_start(3)
    own_start(4)
    second_stage(2, others)
    finish(1)
    each(u_stage)
    finish(2)
    stat_copy.wait()
    for k in range(n_out + 1):
        if k < n_out:
            out_stage(k)
        if k > 0:
            mid_stage(k - 1)
        if k < n_out:
            p_copy(k).start()
        if k > 0:
            a_copy(k - 1).start()
        if 0 < k < n_out - 1:
            nearest(first_stage, 2 + k)
    own_stat[...] = jnp.zeros_like(own_stat)
    own_finish(3)
    own_finish(4)

    def twin_up(k):
        b_copy(k).wait_recv()
        for j in range(n_ffn):
            up_stage(1, k, j)

    def arrive(k):
        for p in down_parts:
            y_copy(p, source(k)).wait_recv()

    second(first_stage, 3)
    nearest(second_stage, 3)
    pass_on(0)
    second(first_stage, 4)
    own_start(5)
    own_start(6)
    nearest(second_stage, 4)
    third(first_stage, 3)
    second(second_stage, 3)
    pass_on(1)
    third(first_stage, 4)
    second(second_stage, 4)
    third(second_stage, 3)
    third(second_stage, 4)
    own_finish(5)
    finish(3)
    own_finish(6)
    finish(4)
    twin_up(0)
    twin_up(1)
    down(0, 0)
    for p in down_parts:
        nearest(first_stage, p)
    pass_on(2)
    each(lambda k: up_stage(0, k, 0))
    merge(0, 0)
    for p in down_parts:
        nearest(second_stage, p)
    arrive(1)
    down(1, 0)
    twin_up(2)
    merge(1, 0)
    each(lambda k: up_stage(0, k, 1))
    pass_on(3)
    for p in down_parts:
        second(first_stage, p)
    twin_up(3)
    down(0, 1)
    down(1, 1)
    merge(0, 1)
    for p in down_parts:
        second(second_stage, p)
    merge(1, 1)
    down(0, None)
    down(1, None)
    arrive(2)
    down(2, 0)
    down(2, 1)
    for p in down_parts:
        third(first_stage, p)
    merge(2, 0)
    merge(2, 1)
    for p in down_parts:
        third(second_stage, p)
    down(2, None)
    arrive(3)
    down(3, 0)
    down(3, 1)
    merge(3, 0)
    merge(3, 1)
    down(3, None)
    each(gather_group)
    s_copy = remote(own_stat, mate_stat.at[1], c_send.at[0, 1], c_recv.at[0, 1], mate)
    s_copy.start()
    drain()
    for k in range(n_out):
        a_copy(k).wait_send()
        b_copy(k).wait_send()

        @pl.when(mine(k))
        def _():
            o_copy(k, 0).wait_send()
            o_copy(k, 1).wait_send()

        @pl.when(jnp.logical_not(mine(k)))
        def _():
            d_copy(k, None).wait_send()
            d_copy(k, 0).wait_send()
            d_copy(k, 1).wait_send()

    s_copy.wait()

    def leave(k):
        r = here(k)
        return pltpu.make_async_copy(x_buf.at[r, pl.ds(0, part)], result.at[r, :], out_sem.at[k])

    @pl.loop(0, n_out)
    def _(k):
        r = here(k)
        power = own_stat[r, 0:1] + mate_stat[1, r, 0:1]
        scale = lax.rsqrt(power / width + 1e-06)
        total = acc[r, :] * scale * gain_ffn_out[:, half_cols]
        x_buf[r, pl.ds(0, part)] = (stream[tp, r, :].astype(single) + total).astype(half)
        leave(k).start()

    for k in range(n_out):
        leave(k).wait()


def rms_norm(values, gain, width, power_sum):
    return values * lax.rsqrt(power_sum / width + 1e-06) * gain


def local(
    resid,
    gain_mix_in,
    u_weight,
    v_weight,
    u_scale,
    v_scale,
    v_gain,
    mix_matrix,
    mix_bias,
    out_weight,
    out_scale,
    gain_mix_out,
    gain_ffn_in,
    up_weight,
    up_scale,
    down_weight,
    down_scale,
    gain_ffn_out,
):
    rows = resid.shape[0]
    part_width = resid.shape[1]
    width = part_width * lax.axis_size("tp")
    lane = lax.axis_index("tp")
    full_rows = lax.all_gather(resid, "tp", axis=1, tiled=True)
    out_scales, down_scales = (
        lax.all_gather(out_scale, "fs", axis=0, tiled=True),
        lax.all_gather(down_scale, "fs", axis=0, tiled=True),
    )
    full_float = full_rows.astype(jnp.float32)
    normed = rms_norm(
        full_float, gain_mix_in, width, jnp.sum(full_float * full_float, axis=1, keepdims=True)
    ).astype(jnp.bfloat16)
    branch_cols = u_weight.shape[1]
    u_pre = jnp.dot(
        normed,
        lax.all_gather(u_weight.astype(jnp.bfloat16), "fs", axis=0, tiled=True),
        preferred_element_type=jnp.float32,
    )
    v_pre = jnp.dot(
        normed,
        lax.all_gather(v_weight.astype(jnp.bfloat16), "fs", axis=0, tiled=True),
        preferred_element_type=jnp.float32,
    )
    u_act = jax.nn.gelu(u_pre * u_scale)
    v_act = jax.nn.gelu(v_pre * v_scale)
    total, squares = lax.psum(
        (jnp.sum(v_act, axis=1, keepdims=True), jnp.sum(v_act * v_act, axis=1, keepdims=True)), "tp"
    )
    branch_width = branch_cols * lax.axis_size("tp")
    centre = total / branch_width
    spread = squares / branch_width - centre * centre
    v_norm = ((v_act - centre) * lax.rsqrt(spread + 1e-06) * v_gain).astype(jnp.bfloat16)
    groups = mix_matrix.shape[0]
    block = mix_matrix.shape[1]
    blocks = v_norm.reshape(rows // block, block, groups, branch_cols // groups)
    mixed = (
        jnp.einsum(
            "gts,bsgd->btgd",
            mix_matrix.astype(jnp.bfloat16),
            blocks,
            preferred_element_type=jnp.float32,
        )
        + mix_bias.T[None, :, :, None]
    )
    gated = (u_act * mixed.reshape(rows, branch_cols)).astype(jnp.bfloat16)
    partial_value = jnp.dot(
        gated,
        lax.all_gather(out_weight.astype(jnp.bfloat16), "fs", axis=1, tiled=True),
        preferred_element_type=jnp.float32,
    )
    mix_out = lax.psum(partial_value.astype(jnp.bfloat16), "tp").astype(jnp.float32) * out_scales
    power = jnp.sum(mix_out * mix_out, axis=1, keepdims=True)
    middle_full = (full_float + rms_norm(mix_out, gain_mix_out, width, power)).astype(jnp.bfloat16)
    middle = lax.dynamic_slice_in_dim(middle_full, lane * part_width, part_width, 1)
    middle_float = middle_full.astype(jnp.float32)
    ffn_in = rms_norm(
        middle_float,
        gain_ffn_in,
        width,
        jnp.sum(middle_float * middle_float, axis=1, keepdims=True),
    ).astype(jnp.bfloat16)
    up_half = up_weight.astype(jnp.bfloat16)
    down_half = down_weight.astype(jnp.bfloat16)
    whole_up = lax.all_gather(up_half, "fs", axis=0, tiled=True)
    raised = jnp.dot(ffn_in, whole_up, preferred_element_type=jnp.float32)
    hidden = jnp.square(jax.nn.relu(raised * up_scale)).astype(jnp.bfloat16)
    whole_down = lax.all_gather(down_half, "fs", axis=1, tiled=True)
    terms = jnp.dot(hidden, whole_down, preferred_element_type=jnp.float32)
    own_down = lax.dynamic_slice_in_dim(down_scales, lane * part_width, part_width, 0)
    ffn_out = (
        lax.psum_scatter(terms.astype(jnp.bfloat16), "tp", scatter_dimension=1, tiled=True).astype(
            jnp.float32
        )
        * own_down
    )
    power_out = lax.psum(jnp.sum(ffn_out * ffn_out, axis=1, keepdims=True), "tp")
    own_gain_out = lax.dynamic_slice_in_dim(gain_ffn_out, lane * part_width, part_width, 0)
    return (middle.astype(jnp.float32) + rms_norm(ffn_out, own_gain_out, width, power_out)).astype(
        jnp.bfloat16
    )


def local_fast(
    resid,
    gain_mix_in,
    u_weight,
    v_weight,
    u_scale,
    v_scale,
    v_gain,
    mix_matrix,
    mix_bias,
    out_weight,
    out_scale,
    gain_mix_out,
    gain_ffn_in,
    up_weight,
    up_scale,
    down_weight,
    down_scale,
    gain_ffn_out,
):
    rows, part = resid.shape
    members = lax.axis_size("fs")
    width = part * 2
    depth, branch = v_weight.shape
    shared = up_weight.shape[1] // 2
    parts = 3 + 2 * (shared // branch)
    n_in = 2
    n_out = members // n_in
    half, single = jnp.bfloat16, jnp.float32
    groups, block = mix_matrix.shape[0], mix_matrix.shape[1]

    def row(vector):
        return vector.reshape(1, -1)

    big = [resid, v_weight, u_weight, out_weight, up_weight, down_weight]
    small = [
        row(gain_mix_in),
        row(u_scale),
        row(v_scale),
        row(v_gain),
        mix_matrix,
        mix_bias,
        row(out_scale),
        row(gain_mix_out),
        row(gain_ffn_in),
        row(up_scale),
        row(down_scale),
        row(gain_ffn_out),
    ]
    dma = pltpu.SemaphoreType.DMA
    scratch = [
        pltpu.VMEM((parts, members, depth, branch), half),
        pltpu.VMEM((rows, part), single),
        pltpu.VMEM((rows, width), half),
        pltpu.VMEM((rows, width), half),
        pltpu.VMEM((2, rows, part), half),
        pltpu.VMEM((2, rows, shared), half),
        pltpu.VMEM((2, rows, width), half),
        pltpu.VMEM((rows, width), half),
        pltpu.VMEM((2, rows, part), half),
        pltpu.VMEM((rows, part), half),
        pltpu.VMEM((rows, 128), single),
        pltpu.VMEM((2, rows, 128), single),
        pltpu.VMEM((groups * block, block), half),
        pltpu.VMEM((block, branch), single),
        dma((parts, 2, n_out)),
        dma((parts, n_out)),
        dma((parts - 3, 2, n_out)),
        dma((parts - 3, n_out)),
        dma((parts, n_out)),
        dma((parts, n_out)),
        dma((3, n_out, 2)),
        dma((3, n_out, 2)),
        dma((parts, branch // depth)),
        dma((2,)),
        dma((2,)),
        dma((n_out, 2)),
        dma((n_out, 2)),
        dma((n_out, 2)),
        dma((n_out, 2)),
        dma((3, n_out)),
        dma((3, n_out)),
        dma((n_out, 2)),
        dma((n_out, 2)),
        dma((n_out,)),
    ]
    return pl.pallas_call(
        functools.partial(fused_kernel, n_out, n_in),
        out_shape=jax.ShapeDtypeStruct((rows, part), half),
        in_specs=[pl.BlockSpec(memory_space=pl.ANY)] * len(big)
        + [pl.BlockSpec(memory_space=pltpu.VMEM)] * len(small),
        out_specs=pl.BlockSpec(memory_space=pl.ANY),
        scratch_shapes=scratch,
        compiler_params=pltpu.CompilerParams(
            collective_id=0, has_side_effects=True, vmem_limit_bytes=63 * 1024 * 1024
        ),
        name="fused_layer",
    )(*big, *small)


def solution(mesh):
    in_specs = (
        P(("rep", "fs"), "tp"),
        P(),
        P("fs", "tp"),
        P("fs", "tp"),
        P("tp"),
        P("tp"),
        P("tp"),
        P("tp", None, None),
        P("tp", None),
        P("tp", "fs"),
        P("fs"),
        P(),
        P(),
        P("fs", "tp"),
        P("tp"),
        P("tp", "fs"),
        P("fs"),
        P(),
    )
    out_specs = P(("rep", "fs"), "tp")
    sizes = mesh.shape

    def whole(*args):
        rows = args[0].shape[0] // (sizes["rep"] * sizes["fs"])
        width = args[0].shape[1]
        branch = args[2].shape[1] // sizes["tp"]
        hidden = args[13].shape[1] // sizes["tp"]
        groups, block = args[7].shape[0] // sizes["tp"], args[7].shape[1]
        planes, depth = sizes["fs"] // 2, width // sizes["fs"]
        paired = sizes["rep"] == 2 and sizes["tp"] == 2 and sizes["fs"] % 4 == 0
        fits = depth % 256 == 0 and branch % depth == 0 and hidden == 4 * branch
        blocks = rows % (planes * block) == 0 and (256 * groups) % branch == 0
        small = 2 * width * (3 * branch + 2 * hidden) <= 24 * 1024 * 1024
        fast = paired and planes == 4 and fits and blocks and small
        return mapped(local_fast if fast else local)(*args)

    def mapped(body):
        return jax.shard_map(
            body, mesh=mesh, in_specs=in_specs, out_specs=out_specs, check_vma=False
        )

    return whole
```

```python
import functools

import jax
import jax.numpy as jnp
from jax import lax
from jax.experimental import pallas as pl
from jax.experimental.pallas import tpu as pltpu
from jax.sharding import PartitionSpec as P


def fused_kernel(n_out, n_in, *refs):
    resid, v_weight, u_weight, out_weight, up_weight, down_weight = refs[:6]
    gain_mix_in, u_scale, v_scale, v_gain, mix_matrix, mix_bias = refs[6:12]
    out_scale, gain_mix_out, gain_ffn_in, up_scale, down_scale, gain_ffn_out = refs[12:18]
    result = refs[18]
    gathered, acc, x_buf, x_twin, stream, h_buf, terms, p_recv, d_recv, o_recv = refs[19:29]
    own_stat, mate_stat, mixers, bias = refs[29:33]
    z_send, z_recv, e_send, e_recv, y_send, y_recv, x_send, x_recv, load_sem = refs[33:42]
    t_send, t_recv, c_send, c_recv, a_send, a_recv, d_send, d_sem, o_send, o_sem, out_sem = refs[
        42:53
    ]
    half, single = jnp.bfloat16, jnp.float32
    parts, members, depth, branch = gathered.shape
    rows, width = x_buf.shape
    part = width // 2
    shared = h_buf.shape[2]
    pieces = branch // depth
    n_ffn = (parts - 3) // 2
    groups, block = mix_matrix.shape[0], mix_matrix.shape[1]
    chunk = rows // n_out
    member = lax.axis_index("fs")
    rep = lax.axis_index("rep")
    tp = lax.axis_index("tp")
    outer, inner = member // n_in, member % n_in
    peer_in = 1 - inner
    cut = 3 * depth // 16
    has_left, has_right = outer > 0, outer < n_out - 1
    across, twin, mate = {"fs": outer * n_in + peer_in}, {"rep": 1 - rep}, {"tp": 1 - tp}

    def greet(device):
        pl.semaphore_signal(barrier, inc=1, device_id=device, device_id_type=pl.DeviceIdType.MESH)

    barrier = pltpu.get_barrier_semaphore()
    for step in (1, n_out - 1):
        greet({"fs": lax.rem(outer + step, n_out) * n_in + inner})
    for device in (across, twin, mate):
        greet(device)

    def remote(src, dst, send, recv, device):
        return pltpu.make_async_remote_copy(
            src_ref=src,
            dst_ref=dst,
            send_sem=send,
            recv_sem=recv,
            device_id=device,
            device_id_type=pl.DeviceIdType.MESH,
        )

    def slot(p, index, base, size):
        return gathered.at[p, index, pl.ds(pl.multiple_of(base, depth // 16), size), :]

    def moved(ref, send, recv, device):
        return remote(ref, ref, send, recv, device)

    def z_copy(p, src, right):
        whole = p >= 3
        base, size = (0, depth) if whole else (rep * (depth // 4), 3 * depth // 4)
        ref = slot(p, src * n_in + inner, base, size)
        way = right.astype(jnp.int32)
        device = {"fs": (outer + 2 * way - 1) * n_in + inner}
        return moved(ref, z_send.at[p, way, src], z_recv.at[p, src], device)

    def e_copy(p, src, right):
        ref = slot(p, src * n_in + peer_in, 0, cut)
        way = right.astype(jnp.int32)
        device = {"fs": (outer + 2 * way - 1) * n_in + inner}
        return moved(ref, e_send.at[p - 3, way, src], e_recv.at[p - 3, src], device)

    def y_copy(p, src):
        base, size = (cut, depth - cut) if p >= 3 else (rep * (depth // 2), depth // 2)
        ref = slot(p, src * n_in + inner, base, size)
        return moved(ref, y_send.at[p, src], y_recv.at[p, src], across)

    def y_own(p):
        base, size = (0, depth) if p >= 3 else (rep * (depth // 8), 7 * depth // 8)
        ref = slot(p, member, base, size)
        return moved(ref, y_send.at[p, outer], y_recv.at[p, outer], across)

    def x_own(p):
        ref = slot(p, outer * n_in + peer_in, rep * (7 * depth // 8), depth // 8)
        return moved(ref, x_send.at[p, outer, 0], x_recv.at[p, outer, 0], twin)

    def x_side(p, src):
        ref = slot(p, src * n_in + inner, rep * (3 * depth // 4), depth // 4)
        return moved(ref, x_send.at[p, src, 0], x_recv.at[p, src, 0], twin)

    def x_diag(p, src):
        ref = slot(p, src * n_in + peer_in, rep * (depth // 2), depth // 2)
        return moved(ref, x_send.at[p, src, 1], x_recv.at[p, src, 1], twin)

    def source(k):
        both = jnp.minimum(outer, n_out - 1 - outer)
        near = k <= 2 * both
        d = jnp.where(near, (k + 1) // 2, k - both)
        long_right = outer < n_out - 1 - outer
        right = jnp.where(near, k % 2 == 0, long_right)
        return jnp.where(right, outer + d, outer - d)

    yes = outer >= 0

    def own_start(p):
        both_ways(z_copy, p, begin)
        y_own(p).start()

    def both_ways(copy, p, act):
        pl.when(has_right)(lambda: act(copy(p, outer, yes)))
        pl.when(has_left)(lambda: act(copy(p, outer, outer < 0)))

    def begin(copy):
        copy.start()

    def own_finish(p):
        y_own(p).wait_recv()
        if p < 3:
            x_own(p).start()
        else:
            both_ways(e_copy, p, begin)

    def onward(src):
        return jnp.where(src < outer, has_right, has_left)

    def first_stage(p, k):
        src = source(k)
        z_copy(p, src, src < outer).wait_recv()
        pl.when(onward(src))(lambda: z_copy(p, src, src < outer).start())
        y_copy(p, src).start()
        if p < 3:
            x_side(p, src).start()

    def second_stage(p, k):
        src = source(k)
        if p < 3:
            y_copy(p, src).wait_recv()
            x_diag(p, src).start()
        else:
            e_copy(p, src, src < outer).wait_recv()
            pl.when(onward(src))(lambda: e_copy(p, src, src < outer).start())

    others = n_out - 1

    def comm(p, k):
        @pl.when(k == 0)
        def _():
            own_finish(p)
            if p > 0:
                second_stage(p - 1, others)

        @pl.when(k > 0)
        def _():
            first_stage(p, k)
            pl.when(k > 1)(lambda: second_stage(p, k - 1))

    def finish(p):
        if p < 3:
            x_own(p).wait_recv()

        @pl.loop(1, n_out)
        def _(k):
            src = source(k)
            if p < 3:
                x_side(p, src).wait_recv()
                x_diag(p, src).wait_recv()
            else:
                y_copy(p, src).wait_recv()

    def settle(copy):
        copy.wait_send()

    def drain():
        for p in range(parts):
            both_ways(z_copy, p, settle)
            y_own(p).wait_send()
            if p < 3:
                x_own(p).wait_send()
            else:
                both_ways(e_copy, p, settle)

            @pl.loop(1, n_out)
            def _(k):
                src = source(k)
                pl.when(onward(src))(lambda: z_copy(p, src, src < outer).wait_send())
                y_copy(p, src).wait_send()
                if p < 3:
                    x_side(p, src).wait_send()
                    x_diag(p, src).wait_send()
                else:
                    pl.when(onward(src))(lambda: e_copy(p, src, src < outer).wait_send())

    def tile(p):
        return pl.ds((p % n_out) * depth, depth), (p // n_out) * branch

    def loads(p):
        low, left = tile(p)
        if p < 2 or 3 <= p < 3 + n_ffn:
            src = (v_weight, u_weight)[p] if p < 2 else up_weight
            first = 0 if p < 2 else rep * shared + (p - 3) * branch
            return [
                pltpu.make_async_copy(
                    src.at[:, pl.ds(first if p < 2 else pl.multiple_of(first, branch), branch)],
                    acc.at[low, pl.ds(left, branch)],
                    load_sem.at[p, 0],
                )
            ]
        src, first = (out_weight, outer * 0) if p == 2 else (down_weight, rep * shared + (p - 3 - n_ffn) * branch)
        return [
            pltpu.make_async_copy(
                src.at[pl.ds(pl.multiple_of(first + i * depth, depth), depth), :],
                acc.at[low, pl.ds(left + i * depth, depth)],
                load_sem.at[p, i],
            )
            for i in range(pieces)
        ]

    def cast(p):
        for copy in loads(p):
            copy.wait()
        low, left = tile(p)
        if p < 2 or 3 <= p < 3 + n_ffn:
            gathered[p, member] = acc[low, pl.ds(left, branch)].astype(half)
            return
        scale = (out_scale if p == 2 else down_scale)[...]
        for i in range(pieces):
            values = acc[low, pl.ds(left + i * depth, depth)] * scale
            gathered[p, member, :, pl.ds(i * depth, depth)] = values.astype(half)

    for p in (0, 1):
        for copy in loads(p):
            copy.start()
    fetch = pltpu.make_async_copy(resid, stream.at[tp], out_sem.at[0])
    fetch.start()
    for p in range(2, parts):
        for copy in loads(p):
            copy.start()
    cast(0)
    cast(1)
    swap = remote(stream.at[tp], stream.at[tp], t_send.at[0], t_recv.at[0], mate)
    pl.semaphore_wait(barrier, 5)
    own_start(0)
    own_start(1)
    fetch.wait()
    swap.start()
    for p in range(2, parts):
        cast(p)
    mixers[...] = mix_matrix[...].reshape(groups * block, block).astype(half)
    span = branch // groups
    turned = mix_bias[...].T
    lanes = lax.broadcasted_iota(jnp.int32, (block, 128), 1)
    for first in range(0, branch, 128):
        column = turned[:, first // span : first // span + 1]
        level = jnp.broadcast_to(column, (block, 128))
        for g in range(first // span + 1, (first + 127) // span + 1):
            level = jnp.where(lanes >= g * span - first, turned[:, g : g + 1], level)
        bias[:, pl.ds(first, 128)] = level
    swap.wait()

    def here(k):
        return pl.ds(pl.multiple_of(k * chunk, chunk), chunk)

    def dot(a, b):
        return jnp.dot(a, b, preferred_element_type=single)

    def spanned(p):
        return gathered[p].reshape(width, branch)

    def norm_stage(k):
        r = here(k)
        a, b = stream[0, r, :].astype(single), stream[1, r, :].astype(single)
        power = jnp.sum(a * a, axis=1, keepdims=True) + jnp.sum(b * b, axis=1, keepdims=True)
        scale = lax.rsqrt(power / width + 1e-06)
        x_buf[r, pl.ds(0, part)] = (a * scale * gain_mix_in[:, :part]).astype(half)
        x_buf[r, pl.ds(part, part)] = (b * scale * gain_mix_in[:, part:]).astype(half)

    def v_stage(k):
        r = here(k)
        act = jax.nn.gelu(dot(x_buf[r, :], spanned(0)) * v_scale[...])
        acc[r, pl.ds(0, branch)] = act
        total = jnp.sum(act, axis=1, keepdims=True)
        squares = jnp.sum(act * act, axis=1, keepdims=True)
        lane = lax.broadcasted_iota(jnp.int32, (chunk, 128), 1)
        own_stat[r, :] = jnp.where(lane == 0, total, squares)

    stat_copy = remote(own_stat, mate_stat.at[0], t_send.at[1], t_recv.at[1], mate)

    def u_stage(k):
        pl.when(k == 0)(lambda: stat_copy.start())
        r = here(k)
        act = jax.nn.gelu(dot(x_buf[r, :], spanned(1)) * u_scale[...])
        acc[r, pl.ds(branch, branch)] = act

    def p_copy(k):
        r = here(k)
        return remote(terms.at[0, r, :], p_recv.at[r, :], c_send.at[k, 0], c_recv.at[k, 0], mate)

    def times(values, p, m):
        total = dot(values[:, :depth], gathered[p, m, :, pl.ds(0, depth)])
        for i in range(1, pieces):
            total += dot(
                values[:, i * depth : (i + 1) * depth], gathered[p, m, :, pl.ds(i * depth, depth)]
            )
        return total

    def out_stage(k):
        r = here(k)
        sums = own_stat[r, :] + mate_stat[0, r, :]
        centre = sums[:, 0:1] / (2 * branch)
        spread = sums[:, 1:2] / (2 * branch) - centre * centre
        scale = lax.rsqrt(spread + 1e-06)
        normed = ((acc[r, pl.ds(0, branch)] - centre) * scale * v_gain[...]).astype(half)
        per = 256 // span
        lane = lax.broadcasted_iota(jnp.int32, (block, 256), 1)
        gates = []
        for b in range(chunk // block):
            line = []
            for q in range(branch // 256):
                both = dot(
                    mixers[pl.ds(q * per * block, per * block), :],
                    normed[b * block : (b + 1) * block, q * 256 : (q + 1) * 256],
                )
                mixed = both[:block]
                for g in range(1, per):
                    mixed = jnp.where(lane >= g * span, both[g * block : (g + 1) * block], mixed)
                line.append(mixed + bias[:, pl.ds(q * 256, 256)])
            gates.append(jnp.concatenate(line, axis=1))
        gate = jnp.concatenate(gates, axis=0)
        gated = (acc[r, pl.ds(branch, branch)] * gate).astype(half)
        for m in range(members):
            terms[0, r, pl.ds(m * depth, depth)] = times(gated, 2, m).astype(half)

    def mid_stage(k):
        p_copy(k).wait()
        r = here(k)
        mix = terms[0, r, :].astype(single) + p_recv[r, :].astype(single)
        scale = lax.rsqrt(jnp.sum(mix * mix, axis=1, keepdims=True) / width + 1e-06)
        mix = mix * scale * gain_mix_out[...]
        a = (stream[0, r, :].astype(single) + mix[:, :part]).astype(half)
        b = (stream[1, r, :].astype(single) + mix[:, part:]).astype(half)
        stream[0, r, :] = a
        stream[1, r, :] = b
        a, b = a.astype(single), b.astype(single)
        power = jnp.sum(a * a, axis=1, keepdims=True) + jnp.sum(b * b, axis=1, keepdims=True)
        scale = lax.rsqrt(power / width + 1e-06)
        x_buf[r, pl.ds(0, part)] = (a * scale * gain_ffn_in[:, :part]).astype(half)
        x_buf[r, pl.ds(part, part)] = (b * scale * gain_ffn_in[:, part:]).astype(half)

    half_cols = pl.ds(pl.multiple_of(tp * part, part), part)

    def a_copy(k):
        r = here(k)
        return remote(
            x_buf.at[r, half_cols], x_twin.at[r, half_cols], a_send.at[k, 0], a_recv.at[k, 0], twin
        )

    def b_copy(k):
        r = here(k)
        return remote(
            x_twin.at[r, half_cols], x_twin.at[r, half_cols], a_send.at[k, 1], a_recv.at[k, 1], mate
        )

    def pass_on(k):
        a_copy(k).wait_recv()
        b_copy(k).start()

    def up_stage(w, k, j):
        r = here(k)
        source_rows = x_twin if w else x_buf
        scale = up_scale[:, pl.ds(pl.multiple_of(rep * shared + j * branch, branch), branch)]
        raised = jax.nn.relu(dot(source_rows[r, :], spanned(3 + j)) * scale)
        h_buf[w, r, pl.ds(j * branch, branch)] = (raised * raised).astype(half)

    planes = n_out // 2
    block_cols = n_in * depth

    def wide(src):
        return pl.ds(pl.multiple_of(src * block_cols, block_cols), block_cols)

    def narrow(src):
        return wide(src % planes)

    early = n_out - 1
    limits = ((0, early), (early, n_out))

    def span_of(q):
        low, high = limits[q]
        return pl.ds(low * chunk, (high - low) * chunk)

    def d_copy(src, q):
        w, r = (0, pl.ds(0, rows)) if q is None else (1, span_of(q))
        lane = 0 if q is None else 1 + q
        return remote(
            terms.at[w, r, wide(src)],
            d_recv.at[w, r, narrow(src)],
            d_send.at[lane, src],
            d_sem.at[lane, src],
            mate,
        )

    def o_copy(src, q):
        r = span_of(q)
        return remote(
            terms.at[1, r, wide(src)],
            o_recv.at[r, narrow(src)],
            o_send.at[src, q],
            o_sem.at[src, q],
            twin,
        )

    def mine(src):
        return src // planes == tp

    def down(k, q):
        src = source(k)
        w, low, high = (0, 0, n_out) if q is None else (1, *limits[q])

        @pl.loop(low, high)
        def _(c):
            r = here(c)
            values = h_buf[w, r, :]
            for i in range(n_in):
                m = src * n_in + i
                total = times(values[:, :branch], 3 + n_ffn, m)
                for j in range(1, n_ffn):
                    total += times(values[:, j * branch : (j + 1) * branch], 3 + n_ffn + j, m)
                cols = pl.ds(pl.multiple_of(m * depth, depth), depth)
                terms[w, r, cols] = total.astype(half)

        pl.when(jnp.logical_not(mine(src)))(lambda: d_copy(src, q).start())

    def merge(k, q):
        src = source(k)

        @pl.when(mine(src))
        def _():
            d_copy(src, q).wait_recv()

            @pl.loop(*limits[q])
            def _(c):
                r = here(c)
                total = terms[1, r, wide(src)].astype(single)
                total += d_recv[1, r, narrow(src)].astype(single)
                terms[1, r, wide(src)] = total.astype(half)

            o_copy(src, q).start()

    def gather_group(k):
        src = source(k)

        @pl.when(mine(src))
        def _():
            d_copy(src, None).wait_recv()
            o_copy(src, 0).wait_recv()
            o_copy(src, 1).wait_recv()

            @pl.loop(0, n_out)
            def _(c):
                r = here(c)
                total = terms[0, r, wide(src)].astype(single)
                total += d_recv[0, r, narrow(src)].astype(single)
                total += o_recv[r, narrow(src)].astype(single)
                acc[r, narrow(src)] = total
                power = jnp.sum(total * total, axis=1, keepdims=True)
                own_stat[r, :] += jnp.broadcast_to(power, (chunk, 128))

    def segment(p, *stages):
        @pl.loop(0, n_out)
        def _(k):
            comm(p, k)
            for stage in stages:
                stage(k)

    def each(stage):
        pl.loop(0, n_out)(stage)

    up_parts = range(3, 3 + n_ffn)
    down_parts = range(3 + n_ffn, parts)
    final = n_out - 1
    middle = jnp.logical_and(has_left, has_right)

    def nearest(stage, p):
        stage(p, 1)
        pl.when(middle)(lambda: stage(p, 2))

    def second(stage, p):
        stage(p, jnp.where(middle, 3, 2))

    def third(stage, p):
        pl.when(jnp.logical_not(middle))(lambda: stage(p, 3))

    segment(0)
    own_start(2)
    segment(1, norm_stage)
    finish(0)
    segment(2, v_stage)
    own_start(3)
    own_start(4)
    second_stage(2, others)
    finish(1)
    each(u_stage)
    finish(2)
    stat_copy.wait()
    for k in range(n_out + 1):
        if k < n_out:
            out_stage(k)
        if k > 0:
            mid_stage(k - 1)
        if k < n_out:
            p_copy(k).start()
        if k > 0:
            a_copy(k - 1).start()
        if 0 < k < n_out - 1:
            nearest(first_stage, 2 + k)
            own_finish(2 + k)
    own_stat[...] = jnp.zeros_like(own_stat)

    def twin_up(k):
        b_copy(k).wait_recv()
        for j in range(n_ffn):
            up_stage(1, k, j)

    def arrive(k):
        for p in down_parts:
            y_copy(p, source(k)).wait_recv()

    nearest(second_stage, 3)
    second(first_stage, 3)
    pass_on(0)
    nearest(second_stage, 4)
    second(first_stage, 4)
    second(second_stage, 3)
    third(first_stage, 3)
    second(second_stage, 4)
    both_ways(z_copy, 5, begin)
    both_ways(z_copy, 6, begin)
    pass_on(1)
    third(first_stage, 4)
    y_own(5).start()
    y_own(6).start()
    third(second_stage, 3)
    third(second_stage, 4)
    finish(3)
    finish(4)
    twin_up(0)
    twin_up(1)
    own_finish(5)
    pass_on(2)
    nearest(first_stage, 5)
    each(lambda k: up_stage(0, k, 0))
    twin_up(2)
    own_finish(6)
    down(0, 0)
    nearest(first_stage, 6)
    merge(0, 0)
    each(lambda k: up_stage(0, k, 1))
    pass_on(3)
    nearest(second_stage, 5)
    nearest(second_stage, 6)
    twin_up(3)
    down(0, 1)
    arrive(1)
    down(1, 0)
    merge(0, 1)
    second(first_stage, 5)
    down(1, 1)
    merge(1, 0)
    merge(1, 1)
    second(first_stage, 6)
    down(0, None)
    second(second_stage, 5)
    second(second_stage, 6)
    third(first_stage, 5)
    arrive(2)
    down(2, 0)
    down(2, 1)
    merge(2, 0)
    merge(2, 1)
    third(first_stage, 6)
    down(1, None)
    third(second_stage, 5)
    third(second_stage, 6)
    down(2, None)
    arrive(3)
    down(3, 0)
    down(3, 1)
    merge(3, 0)
    merge(3, 1)
    down(3, None)
    each(gather_group)
    s_copy = remote(own_stat, mate_stat.at[1], c_send.at[0, 1], c_recv.at[0, 1], mate)
    s_copy.start()
    drain()
    for k in range(n_out):
        a_copy(k).wait_send()
        b_copy(k).wait_send()

        @pl.when(mine(k))
        def _():
            o_copy(k, 0).wait_send()
            o_copy(k, 1).wait_send()

        @pl.when(jnp.logical_not(mine(k)))
        def _():
            d_copy(k, None).wait_send()
            d_copy(k, 0).wait_send()
            d_copy(k, 1).wait_send()

    s_copy.wait()

    def leave(k):
        r = here(k)
        return pltpu.make_async_copy(x_buf.at[r, pl.ds(0, part)], result.at[r, :], out_sem.at[k])

    @pl.loop(0, n_out)
    def _(k):
        r = here(k)
        power = own_stat[r, 0:1] + mate_stat[1, r, 0:1]
        scale = lax.rsqrt(power / width + 1e-06)
        total = acc[r, :] * scale * gain_ffn_out[:, half_cols]
        x_buf[r, pl.ds(0, part)] = (stream[tp, r, :].astype(single) + total).astype(half)
        leave(k).start()

    for k in range(n_out):
        leave(k).wait()


def rms_norm(values, gain, width, power_sum):
    return values * lax.rsqrt(power_sum / width + 1e-06) * gain


def local(
    resid,
    gain_mix_in,
    u_weight,
    v_weight,
    u_scale,
    v_scale,
    v_gain,
    mix_matrix,
    mix_bias,
    out_weight,
    out_scale,
    gain_mix_out,
    gain_ffn_in,
    up_weight,
    up_scale,
    down_weight,
    down_scale,
    gain_ffn_out,
):
    rows = resid.shape[0]
    part_width = resid.shape[1]
    width = part_width * lax.axis_size("tp")
    lane = lax.axis_index("tp")
    full_rows = lax.all_gather(resid, "tp", axis=1, tiled=True)
    out_scales, down_scales = (
        lax.all_gather(out_scale, "fs", axis=0, tiled=True),
        lax.all_gather(down_scale, "fs", axis=0, tiled=True),
    )
    full_float = full_rows.astype(jnp.float32)
    normed = rms_norm(
        full_float, gain_mix_in, width, jnp.sum(full_float * full_float, axis=1, keepdims=True)
    ).astype(jnp.bfloat16)
    branch_cols = u_weight.shape[1]
    u_pre = jnp.dot(
        normed,
        lax.all_gather(u_weight.astype(jnp.bfloat16), "fs", axis=0, tiled=True),
        preferred_element_type=jnp.float32,
    )
    v_pre = jnp.dot(
        normed,
        lax.all_gather(v_weight.astype(jnp.bfloat16), "fs", axis=0, tiled=True),
        preferred_element_type=jnp.float32,
    )
    u_act = jax.nn.gelu(u_pre * u_scale)
    v_act = jax.nn.gelu(v_pre * v_scale)
    total, squares = lax.psum(
        (jnp.sum(v_act, axis=1, keepdims=True), jnp.sum(v_act * v_act, axis=1, keepdims=True)), "tp"
    )
    branch_width = branch_cols * lax.axis_size("tp")
    centre = total / branch_width
    spread = squares / branch_width - centre * centre
    v_norm = ((v_act - centre) * lax.rsqrt(spread + 1e-06) * v_gain).astype(jnp.bfloat16)
    groups = mix_matrix.shape[0]
    block = mix_matrix.shape[1]
    blocks = v_norm.reshape(rows // block, block, groups, branch_cols // groups)
    mixed = (
        jnp.einsum(
            "gts,bsgd->btgd",
            mix_matrix.astype(jnp.bfloat16),
            blocks,
            preferred_element_type=jnp.float32,
        )
        + mix_bias.T[None, :, :, None]
    )
    gated = (u_act * mixed.reshape(rows, branch_cols)).astype(jnp.bfloat16)
    partial_value = jnp.dot(
        gated,
        lax.all_gather(out_weight.astype(jnp.bfloat16), "fs", axis=1, tiled=True),
        preferred_element_type=jnp.float32,
    )
    mix_out = lax.psum(partial_value.astype(jnp.bfloat16), "tp").astype(jnp.float32) * out_scales
    power = jnp.sum(mix_out * mix_out, axis=1, keepdims=True)
    middle_full = (full_float + rms_norm(mix_out, gain_mix_out, width, power)).astype(jnp.bfloat16)
    middle = lax.dynamic_slice_in_dim(middle_full, lane * part_width, part_width, 1)
    middle_float = middle_full.astype(jnp.float32)
    ffn_in = rms_norm(
        middle_float,
        gain_ffn_in,
        width,
        jnp.sum(middle_float * middle_float, axis=1, keepdims=True),
    ).astype(jnp.bfloat16)
    up_half = up_weight.astype(jnp.bfloat16)
    down_half = down_weight.astype(jnp.bfloat16)
    whole_up = lax.all_gather(up_half, "fs", axis=0, tiled=True)
    raised = jnp.dot(ffn_in, whole_up, preferred_element_type=jnp.float32)
    hidden = jnp.square(jax.nn.relu(raised * up_scale)).astype(jnp.bfloat16)
    whole_down = lax.all_gather(down_half, "fs", axis=1, tiled=True)
    terms = jnp.dot(hidden, whole_down, preferred_element_type=jnp.float32)
    own_down = lax.dynamic_slice_in_dim(down_scales, lane * part_width, part_width, 0)
    ffn_out = (
        lax.psum_scatter(terms.astype(jnp.bfloat16), "tp", scatter_dimension=1, tiled=True).astype(
            jnp.float32
        )
        * own_down
    )
    power_out = lax.psum(jnp.sum(ffn_out * ffn_out, axis=1, keepdims=True), "tp")
    own_gain_out = lax.dynamic_slice_in_dim(gain_ffn_out, lane * part_width, part_width, 0)
    return (middle.astype(jnp.float32) + rms_norm(ffn_out, own_gain_out, width, power_out)).astype(
        jnp.bfloat16
    )


def local_fast(
    resid,
    gain_mix_in,
    u_weight,
    v_weight,
    u_scale,
    v_scale,
    v_gain,
    mix_matrix,
    mix_bias,
    out_weight,
    out_scale,
    gain_mix_out,
    gain_ffn_in,
    up_weight,
    up_scale,
    down_weight,
    down_scale,
    gain_ffn_out,
):
    rows, part = resid.shape
    members = lax.axis_size("fs")
    width = part * 2
    depth, branch = v_weight.shape
    shared = up_weight.shape[1] // 2
    parts = 3 + 2 * (shared // branch)
    n_in = 2
    n_out = members // n_in
    half, single = jnp.bfloat16, jnp.float32
    groups, block = mix_matrix.shape[0], mix_matrix.shape[1]

    def row(vector):
        return vector.reshape(1, -1)

    big = [resid, v_weight, u_weight, out_weight, up_weight, down_weight]
    small = [
        row(gain_mix_in),
        row(u_scale),
        row(v_scale),
        row(v_gain),
        mix_matrix,
        mix_bias,
        row(out_scale),
        row(gain_mix_out),
        row(gain_ffn_in),
        row(up_scale),
        row(down_scale),
        row(gain_ffn_out),
    ]
    dma = pltpu.SemaphoreType.DMA
    scratch = [
        pltpu.VMEM((parts, members, depth, branch), half),
        pltpu.VMEM((rows, part), single),
        pltpu.VMEM((rows, width), half),
        pltpu.VMEM((rows, width), half),
        pltpu.VMEM((2, rows, part), half),
        pltpu.VMEM((2, rows, shared), half),
        pltpu.VMEM((2, rows, width), half),
        pltpu.VMEM((rows, width), half),
        pltpu.VMEM((2, rows, part), half),
        pltpu.VMEM((rows, part), half),
        pltpu.VMEM((rows, 128), single),
        pltpu.VMEM((2, rows, 128), single),
        pltpu.VMEM((groups * block, block), half),
        pltpu.VMEM((block, branch), single),
        dma((parts, 2, n_out)),
        dma((parts, n_out)),
        dma((parts - 3, 2, n_out)),
        dma((parts - 3, n_out)),
        dma((parts, n_out)),
        dma((parts, n_out)),
        dma((3, n_out, 2)),
        dma((3, n_out, 2)),
        dma((parts, branch // depth)),
        dma((2,)),
        dma((2,)),
        dma((n_out, 2)),
        dma((n_out, 2)),
        dma((n_out, 2)),
        dma((n_out, 2)),
        dma((3, n_out)),
        dma((3, n_out)),
        dma((n_out, 2)),
        dma((n_out, 2)),
        dma((n_out,)),
    ]
    return pl.pallas_call(
        functools.partial(fused_kernel, n_out, n_in),
        out_shape=jax.ShapeDtypeStruct((rows, part), half),
        in_specs=[pl.BlockSpec(memory_space=pl.ANY)] * len(big)
        + [pl.BlockSpec(memory_space=pltpu.VMEM)] * len(small),
        out_specs=pl.BlockSpec(memory_space=pl.ANY),
        scratch_shapes=scratch,
        compiler_params=pltpu.CompilerParams(
            collective_id=0, has_side_effects=True, vmem_limit_bytes=63 * 1024 * 1024
        ),
        name="fused_layer",
    )(*big, *small)


def solution(mesh):
    in_specs = (
        P(("rep", "fs"), "tp"),
        P(),
        P("fs", "tp"),
        P("fs", "tp"),
        P("tp"),
        P("tp"),
        P("tp"),
        P("tp", None, None),
        P("tp", None),
        P("tp", "fs"),
        P("fs"),
        P(),
        P(),
        P("fs", "tp"),
        P("tp"),
        P("tp", "fs"),
        P("fs"),
        P(),
    )
    out_specs = P(("rep", "fs"), "tp")
    sizes = mesh.shape

    def whole(*args):
        rows = args[0].shape[0] // (sizes["rep"] * sizes["fs"])
        width = args[0].shape[1]
        branch = args[2].shape[1] // sizes["tp"]
        hidden = args[13].shape[1] // sizes["tp"]
        groups, block = args[7].shape[0] // sizes["tp"], args[7].shape[1]
        planes, depth = sizes["fs"] // 2, width // sizes["fs"]
        paired = sizes["rep"] == 2 and sizes["tp"] == 2 and sizes["fs"] % 4 == 0
        fits = depth % 256 == 0 and branch % depth == 0 and hidden == 4 * branch
        blocks = rows % (planes * block) == 0 and (256 * groups) % branch == 0
        small = 2 * width * (3 * branch + 2 * hidden) <= 24 * 1024 * 1024
        fast = paired and planes == 4 and fits and blocks and small
        return mapped(local_fast if fast else local)(*args)

    def mapped(body):
        return jax.shard_map(
            body, mesh=mesh, in_specs=in_specs, out_specs=out_specs, check_vma=False
        )

    return whole
```

```python
import functools

import jax
import jax.numpy as jnp
from jax import lax
from jax.experimental import pallas as pl
from jax.experimental.pallas import tpu as pltpu
from jax.sharding import PartitionSpec as P


def fused_kernel(n_out, n_in, *refs):
    resid, v_weight, u_weight, out_weight, up_weight, down_weight = refs[:6]
    gain_mix_in, u_scale, v_scale, v_gain, mix_matrix, mix_bias = refs[6:12]
    out_scale, gain_mix_out, gain_ffn_in, up_scale, down_scale, gain_ffn_out = refs[12:18]
    result = refs[18]
    gathered, acc, x_buf, x_twin, stream, h_buf, terms, p_recv, d_recv, o_recv = refs[19:29]
    own_stat, mate_stat, mixers, bias = refs[29:33]
    z_send, z_recv, e_send, e_recv, y_send, y_recv, x_send, x_recv, load_sem = refs[33:42]
    t_send, t_recv, c_send, c_recv, a_send, a_recv, d_send, d_sem, o_send, o_sem, out_sem = refs[
        42:53
    ]
    half, single = jnp.bfloat16, jnp.float32
    parts, members, depth, branch = gathered.shape
    rows, width = x_buf.shape
    part = width // 2
    shared = h_buf.shape[2]
    pieces = branch // depth
    n_ffn = (parts - 3) // 2
    groups, block = mix_matrix.shape[0], mix_matrix.shape[1]
    chunk = rows // n_out
    member = lax.axis_index("fs")
    rep = lax.axis_index("rep")
    tp = lax.axis_index("tp")
    outer, inner = member // n_in, member % n_in
    peer_in = 1 - inner
    cut = 3 * depth // 16
    has_left, has_right = outer > 0, outer < n_out - 1
    across, twin, mate = {"fs": outer * n_in + peer_in}, {"rep": 1 - rep}, {"tp": 1 - tp}

    def greet(device):
        pl.semaphore_signal(barrier, inc=1, device_id=device, device_id_type=pl.DeviceIdType.MESH)

    barrier = pltpu.get_barrier_semaphore()
    for step in (1, n_out - 1):
        greet({"fs": lax.rem(outer + step, n_out) * n_in + inner})
    for device in (across, twin, mate):
        greet(device)

    def remote(src, dst, send, recv, device):
        return pltpu.make_async_remote_copy(
            src_ref=src,
            dst_ref=dst,
            send_sem=send,
            recv_sem=recv,
            device_id=device,
            device_id_type=pl.DeviceIdType.MESH,
        )

    def slot(p, index, base, size):
        return gathered.at[p, index, pl.ds(pl.multiple_of(base, depth // 16), size), :]

    def moved(ref, send, recv, device):
        return remote(ref, ref, send, recv, device)

    def z_copy(p, src, right):
        whole = p >= 3
        base, size = (0, depth) if whole else (rep * (depth // 4), 3 * depth // 4)
        ref = slot(p, src * n_in + inner, base, size)
        way = right.astype(jnp.int32)
        device = {"fs": (outer + 2 * way - 1) * n_in + inner}
        return moved(ref, z_send.at[p, way, src], z_recv.at[p, src], device)

    def e_copy(p, src, right):
        ref = slot(p, src * n_in + peer_in, 0, cut)
        way = right.astype(jnp.int32)
        device = {"fs": (outer + 2 * way - 1) * n_in + inner}
        return moved(ref, e_send.at[p - 3, way, src], e_recv.at[p - 3, src], device)

    def y_copy(p, src):
        base, size = (cut, depth - cut) if p >= 3 else (rep * (depth // 2), depth // 2)
        ref = slot(p, src * n_in + inner, base, size)
        return moved(ref, y_send.at[p, src], y_recv.at[p, src], across)

    def y_own(p):
        base, size = (0, depth) if p >= 3 else (rep * (depth // 8), 7 * depth // 8)
        ref = slot(p, member, base, size)
        return moved(ref, y_send.at[p, outer], y_recv.at[p, outer], across)

    def x_own(p):
        ref = slot(p, outer * n_in + peer_in, rep * (7 * depth // 8), depth // 8)
        return moved(ref, x_send.at[p, outer, 0], x_recv.at[p, outer, 0], twin)

    def x_side(p, src):
        ref = slot(p, src * n_in + inner, rep * (3 * depth // 4), depth // 4)
        return moved(ref, x_send.at[p, src, 0], x_recv.at[p, src, 0], twin)

    def x_diag(p, src):
        ref = slot(p, src * n_in + peer_in, rep * (depth // 2), depth // 2)
        return moved(ref, x_send.at[p, src, 1], x_recv.at[p, src, 1], twin)

    def source(k):
        both = jnp.minimum(outer, n_out - 1 - outer)
        near = k <= 2 * both
        d = jnp.where(near, (k + 1) // 2, k - both)
        long_right = outer < n_out - 1 - outer
        right = jnp.where(near, k % 2 == 0, long_right)
        return jnp.where(right, outer + d, outer - d)

    yes = outer >= 0

    def own_start(p):
        both_ways(z_copy, p, begin)
        y_own(p).start()

    def both_ways(copy, p, act):
        pl.when(has_right)(lambda: act(copy(p, outer, yes)))
        pl.when(has_left)(lambda: act(copy(p, outer, outer < 0)))

    def begin(copy):
        copy.start()

    def own_finish(p):
        y_own(p).wait_recv()
        if p < 3:
            x_own(p).start()
        else:
            both_ways(e_copy, p, begin)

    def onward(src):
        return jnp.where(src < outer, has_right, has_left)

    def first_stage(p, k):
        src = source(k)
        z_copy(p, src, src < outer).wait_recv()
        pl.when(onward(src))(lambda: z_copy(p, src, src < outer).start())
        y_copy(p, src).start()
        if p < 3:
            x_side(p, src).start()

    def second_stage(p, k):
        src = source(k)
        if p < 3:
            y_copy(p, src).wait_recv()
            x_diag(p, src).start()
        else:
            e_copy(p, src, src < outer).wait_recv()
            pl.when(onward(src))(lambda: e_copy(p, src, src < outer).start())

    others = n_out - 1

    def comm(p, k):
        @pl.when(k == 0)
        def _():
            own_finish(p)
            if p > 0:
                second_stage(p - 1, others)

        @pl.when(k > 0)
        def _():
            first_stage(p, k)
            pl.when(k > 1)(lambda: second_stage(p, k - 1))

    def finish(p):
        if p < 3:
            x_own(p).wait_recv()

        @pl.loop(1, n_out)
        def _(k):
            src = source(k)
            if p < 3:
                x_side(p, src).wait_recv()
                x_diag(p, src).wait_recv()
            else:
                y_copy(p, src).wait_recv()

    def settle(copy):
        copy.wait_send()

    def drain():
        for p in range(parts):
            both_ways(z_copy, p, settle)
            y_own(p).wait_send()
            if p < 3:
                x_own(p).wait_send()
            else:
                both_ways(e_copy, p, settle)

            @pl.loop(1, n_out)
            def _(k):
                src = source(k)
                pl.when(onward(src))(lambda: z_copy(p, src, src < outer).wait_send())
                y_copy(p, src).wait_send()
                if p < 3:
                    x_side(p, src).wait_send()
                    x_diag(p, src).wait_send()
                else:
                    pl.when(onward(src))(lambda: e_copy(p, src, src < outer).wait_send())

    def tile(p):
        return pl.ds((p % n_out) * depth, depth), (p // n_out) * branch

    def loads(p):
        low, left = tile(p)
        if p < 2 or 3 <= p < 3 + n_ffn:
            src = (v_weight, u_weight)[p] if p < 2 else up_weight
            first = 0 if p < 2 else rep * shared + (p - 3) * branch
            return [
                pltpu.make_async_copy(
                    src.at[:, pl.ds(first if p < 2 else pl.multiple_of(first, branch), branch)],
                    acc.at[low, pl.ds(left, branch)],
                    load_sem.at[p, 0],
                )
            ]
        src, first = (out_weight, outer * 0) if p == 2 else (down_weight, rep * shared + (p - 3 - n_ffn) * branch)
        return [
            pltpu.make_async_copy(
                src.at[pl.ds(pl.multiple_of(first + i * depth, depth), depth), :],
                acc.at[low, pl.ds(left + i * depth, depth)],
                load_sem.at[p, i],
            )
            for i in range(pieces)
        ]

    def cast(p):
        for copy in loads(p):
            copy.wait()
        low, left = tile(p)
        if p < 2 or 3 <= p < 3 + n_ffn:
            gathered[p, member] = acc[low, pl.ds(left, branch)].astype(half)
            return
        scale = (out_scale if p == 2 else down_scale)[...]
        for i in range(pieces):
            values = acc[low, pl.ds(left + i * depth, depth)] * scale
            gathered[p, member, :, pl.ds(i * depth, depth)] = values.astype(half)

    for p in (0, 1):
        for copy in loads(p):
            copy.start()
    fetch = pltpu.make_async_copy(resid, stream.at[tp], out_sem.at[0])
    fetch.start()
    for p in range(2, parts):
        for copy in loads(p):
            copy.start()
    cast(0)
    cast(1)
    swap = remote(stream.at[tp], stream.at[tp], t_send.at[0], t_recv.at[0], mate)
    pl.semaphore_wait(barrier, 5)
    own_start(0)
    own_start(1)
    fetch.wait()
    swap.start()
    for p in range(2, parts):
        cast(p)
    mixers[...] = mix_matrix[...].reshape(groups * block, block).astype(half)
    span = branch // groups
    turned = mix_bias[...].T
    lanes = lax.broadcasted_iota(jnp.int32, (block, 128), 1)
    for first in range(0, branch, 128):
        column = turned[:, first // span : first // span + 1]
        level = jnp.broadcast_to(column, (block, 128))
        for g in range(first // span + 1, (first + 127) // span + 1):
            level = jnp.where(lanes >= g * span - first, turned[:, g : g + 1], level)
        bias[:, pl.ds(first, 128)] = level
    swap.wait()

    def here(k):
        return pl.ds(pl.multiple_of(k * chunk, chunk), chunk)

    def dot(a, b):
        return jnp.dot(a, b, preferred_element_type=single)

    def spanned(p):
        return gathered[p].reshape(width, branch)

    def norm_stage(k):
        r = here(k)
        a, b = stream[0, r, :].astype(single), stream[1, r, :].astype(single)
        power = jnp.sum(a * a, axis=1, keepdims=True) + jnp.sum(b * b, axis=1, keepdims=True)
        scale = lax.rsqrt(power / width + 1e-06)
        x_buf[r, pl.ds(0, part)] = (a * scale * gain_mix_in[:, :part]).astype(half)
        x_buf[r, pl.ds(part, part)] = (b * scale * gain_mix_in[:, part:]).astype(half)

    def v_stage(k):
        r = here(k)
        act = jax.nn.gelu(dot(x_buf[r, :], spanned(0)) * v_scale[...])
        acc[r, pl.ds(0, branch)] = act
        total = jnp.sum(act, axis=1, keepdims=True)
        squares = jnp.sum(act * act, axis=1, keepdims=True)
        lane = lax.broadcasted_iota(jnp.int32, (chunk, 128), 1)
        own_stat[r, :] = jnp.where(lane == 0, total, squares)

    stat_copy = remote(own_stat, mate_stat.at[0], t_send.at[1], t_recv.at[1], mate)

    def u_stage(k):
        pl.when(k == 0)(lambda: stat_copy.start())
        r = here(k)
        act = jax.nn.gelu(dot(x_buf[r, :], spanned(1)) * u_scale[...])
        acc[r, pl.ds(branch, branch)] = act

    def p_copy(k):
        r = here(k)
        return remote(terms.at[0, r, :], p_recv.at[r, :], c_send.at[k, 0], c_recv.at[k, 0], mate)

    def times(values, p, m):
        total = dot(values[:, :depth], gathered[p, m, :, pl.ds(0, depth)])
        for i in range(1, pieces):
            total += dot(
                values[:, i * depth : (i + 1) * depth], gathered[p, m, :, pl.ds(i * depth, depth)]
            )
        return total

    def out_stage(k):
        r = here(k)
        sums = own_stat[r, :] + mate_stat[0, r, :]
        centre = sums[:, 0:1] / (2 * branch)
        spread = sums[:, 1:2] / (2 * branch) - centre * centre
        scale = lax.rsqrt(spread + 1e-06)
        normed = ((acc[r, pl.ds(0, branch)] - centre) * scale * v_gain[...]).astype(half)
        per = 256 // span
        lane = lax.broadcasted_iota(jnp.int32, (block, 256), 1)
        gates = []
        for b in range(chunk // block):
            line = []
            for q in range(branch // 256):
                both = dot(
                    mixers[pl.ds(q * per * block, per * block), :],
                    normed[b * block : (b + 1) * block, q * 256 : (q + 1) * 256],
                )
                mixed = both[:block]
                for g in range(1, per):
                    mixed = jnp.where(lane >= g * span, both[g * block : (g + 1) * block], mixed)
                line.append(mixed + bias[:, pl.ds(q * 256, 256)])
            gates.append(jnp.concatenate(line, axis=1))
        gate = jnp.concatenate(gates, axis=0)
        gated = (acc[r, pl.ds(branch, branch)] * gate).astype(half)
        for m in range(members):
            terms[0, r, pl.ds(m * depth, depth)] = times(gated, 2, m).astype(half)

    def mid_stage(k):
        p_copy(k).wait()
        r = here(k)
        mix = terms[0, r, :].astype(single) + p_recv[r, :].astype(single)
        scale = lax.rsqrt(jnp.sum(mix * mix, axis=1, keepdims=True) / width + 1e-06)
        mix = mix * scale * gain_mix_out[...]
        a = (stream[0, r, :].astype(single) + mix[:, :part]).astype(half)
        b = (stream[1, r, :].astype(single) + mix[:, part:]).astype(half)
        stream[0, r, :] = a
        stream[1, r, :] = b
        a, b = a.astype(single), b.astype(single)
        power = jnp.sum(a * a, axis=1, keepdims=True) + jnp.sum(b * b, axis=1, keepdims=True)
        scale = lax.rsqrt(power / width + 1e-06)
        x_buf[r, pl.ds(0, part)] = (a * scale * gain_ffn_in[:, :part]).astype(half)
        x_buf[r, pl.ds(part, part)] = (b * scale * gain_ffn_in[:, part:]).astype(half)

    half_cols = pl.ds(pl.multiple_of(tp * part, part), part)

    def a_copy(k):
        r = here(k)
        return remote(
            x_buf.at[r, half_cols], x_twin.at[r, half_cols], a_send.at[k, 0], a_recv.at[k, 0], twin
        )

    def b_copy(k):
        r = here(k)
        return remote(
            x_twin.at[r, half_cols], x_twin.at[r, half_cols], a_send.at[k, 1], a_recv.at[k, 1], mate
        )

    def pass_on(k):
        a_copy(k).wait_recv()
        b_copy(k).start()

    def up_stage(w, k, j):
        r = here(k)
        source_rows = x_twin if w else x_buf
        scale = up_scale[:, pl.ds(pl.multiple_of(rep * shared + j * branch, branch), branch)]
        raised = jax.nn.relu(dot(source_rows[r, :], spanned(3 + j)) * scale)
        h_buf[w, r, pl.ds(j * branch, branch)] = (raised * raised).astype(half)

    planes = n_out // 2
    block_cols = n_in * depth

    def wide(src):
        return pl.ds(pl.multiple_of(src * block_cols, block_cols), block_cols)

    def narrow(src):
        return wide(src % planes)

    early = n_out - 1
    limits = ((0, early), (early, n_out))

    def span_of(q):
        low, high = limits[q]
        return pl.ds(low * chunk, (high - low) * chunk)

    def d_copy(src, q):
        w, r = (0, pl.ds(0, rows)) if q is None else (1, span_of(q))
        lane = 0 if q is None else 1 + q
        return remote(
            terms.at[w, r, wide(src)],
            d_recv.at[w, r, narrow(src)],
            d_send.at[lane, src],
            d_sem.at[lane, src],
            mate,
        )

    def o_copy(src, q):
        r = span_of(q)
        return remote(
            terms.at[1, r, wide(src)],
            o_recv.at[r, narrow(src)],
            o_send.at[src, q],
            o_sem.at[src, q],
            twin,
        )

    def mine(src):
        return src // planes == tp

    def down(k, q):
        src = source(k)
        w, low, high = (0, 0, n_out) if q is None else (1, *limits[q])

        @pl.loop(low, high)
        def _(c):
            r = here(c)
            values = h_buf[w, r, :]
            for i in range(n_in):
                m = src * n_in + i
                total = times(values[:, :branch], 3 + n_ffn, m)
                for j in range(1, n_ffn):
                    total += times(values[:, j * branch : (j + 1) * branch], 3 + n_ffn + j, m)
                cols = pl.ds(pl.multiple_of(m * depth, depth), depth)
                terms[w, r, cols] = total.astype(half)

        pl.when(jnp.logical_not(mine(src)))(lambda: d_copy(src, q).start())

    def merge(k, q):
        src = source(k)

        @pl.when(mine(src))
        def _():
            d_copy(src, q).wait_recv()

            @pl.loop(*limits[q])
            def _(c):
                r = here(c)
                total = terms[1, r, wide(src)].astype(single)
                total += d_recv[1, r, narrow(src)].astype(single)
                terms[1, r, wide(src)] = total.astype(half)

            o_copy(src, q).start()

    def gather_group(k, q):
        src = source(k)

        @pl.when(mine(src))
        def _():
            if q == 0:
                d_copy(src, None).wait_recv()
            o_copy(src, q).wait_recv()

            @pl.loop(*limits[q])
            def _(c):
                r = here(c)
                total = terms[0, r, wide(src)].astype(single)
                total += d_recv[0, r, narrow(src)].astype(single)
                total += o_recv[r, narrow(src)].astype(single)
                acc[r, narrow(src)] = total
                power = jnp.sum(total * total, axis=1, keepdims=True)
                own_stat[r, :] += jnp.broadcast_to(power, (chunk, 128))

    def segment(p, *stages):
        @pl.loop(0, n_out)
        def _(k):
            comm(p, k)
            for stage in stages:
                stage(k)

    def each(stage):
        pl.loop(0, n_out)(stage)

    up_parts = range(3, 3 + n_ffn)
    down_parts = range(3 + n_ffn, parts)
    final = n_out - 1
    middle = jnp.logical_and(has_left, has_right)

    def nearest(stage, p):
        stage(p, 1)
        pl.when(middle)(lambda: stage(p, 2))

    def second(stage, p):
        stage(p, jnp.where(middle, 3, 2))

    def third(stage, p):
        pl.when(jnp.logical_not(middle))(lambda: stage(p, 3))

    segment(0)
    own_start(2)
    segment(1, norm_stage)
    finish(0)
    segment(2, v_stage)
    own_start(3)
    own_start(4)
    second_stage(2, others)
    finish(1)
    each(u_stage)
    finish(2)
    stat_copy.wait()
    for k in range(n_out + 1):
        if k < n_out:
            out_stage(k)
        if k > 0:
            mid_stage(k - 1)
        if k < n_out:
            p_copy(k).start()
        if k > 0:
            a_copy(k - 1).start()
        if 0 < k < n_out - 1:
            nearest(first_stage, 2 + k)
            own_finish(2 + k)
    own_stat[...] = jnp.zeros_like(own_stat)

    def twin_up(k):
        b_copy(k).wait_recv()
        for j in range(n_ffn):
            up_stage(1, k, j)

    def arrive(k):
        for p in down_parts:
            y_copy(p, source(k)).wait_recv()

    nearest(second_stage, 3)
    second(first_stage, 3)
    pass_on(0)
    nearest(second_stage, 4)
    second(first_stage, 4)
    second(second_stage, 3)
    third(first_stage, 3)
    second(second_stage, 4)
    both_ways(z_copy, 5, begin)
    both_ways(z_copy, 6, begin)
    pass_on(1)
    third(first_stage, 4)
    y_own(5).start()
    y_own(6).start()
    third(second_stage, 3)
    third(second_stage, 4)
    finish(3)
    finish(4)
    twin_up(0)
    twin_up(1)
    own_finish(5)
    pass_on(2)
    nearest(first_stage, 5)
    each(lambda k: up_stage(0, k, 0))
    twin_up(2)
    own_finish(6)
    down(0, 0)
    nearest(first_stage, 6)
    merge(0, 0)
    each(lambda k: up_stage(0, k, 1))
    pass_on(3)
    nearest(second_stage, 5)
    nearest(second_stage, 6)
    twin_up(3)
    down(0, 1)
    arrive(1)
    down(1, 0)
    merge(0, 1)
    second(first_stage, 5)
    down(1, 1)
    merge(1, 0)
    merge(1, 1)
    second(first_stage, 6)
    down(0, None)
    second(second_stage, 5)
    second(second_stage, 6)
    third(first_stage, 5)
    arrive(2)
    down(2, 0)
    down(2, 1)
    merge(2, 0)
    merge(2, 1)
    third(first_stage, 6)
    down(1, None)
    third(second_stage, 5)
    third(second_stage, 6)
    down(2, None)
    arrive(3)
    down(3, 0)
    down(3, 1)
    merge(3, 0)
    merge(3, 1)
    down(3, None)
    drain()

    def s_copy(q):
        r = span_of(q)
        return remote(
            own_stat.at[r, :], mate_stat.at[1, r, :], c_send.at[q, 1], c_recv.at[q, 1], mate
        )

    def leave(k):
        r = here(k)
        return pltpu.make_async_copy(x_buf.at[r, pl.ds(0, part)], result.at[r, :], out_sem.at[k])

    for k in range(n_out):
        a_copy(k).wait_send()
        b_copy(k).wait_send()

    for q in range(2):
        each(lambda k: gather_group(k, q))
        s_copy(q).start()
        s_copy(q).wait()

        @pl.loop(*limits[q])
        def _(k):
            r = here(k)
            power = own_stat[r, 0:1] + mate_stat[1, r, 0:1]
            scale = lax.rsqrt(power / width + 1e-06)
            total = acc[r, :] * scale * gain_ffn_out[:, half_cols]
            x_buf[r, pl.ds(0, part)] = (stream[tp, r, :].astype(single) + total).astype(half)
            leave(k).start()

    for k in range(n_out):

        @pl.when(mine(k))
        def _():
            o_copy(k, 0).wait_send()
            o_copy(k, 1).wait_send()

        @pl.when(jnp.logical_not(mine(k)))
        def _():
            d_copy(k, None).wait_send()
            d_copy(k, 0).wait_send()
            d_copy(k, 1).wait_send()

    for k in range(n_out):
        leave(k).wait()


def rms_norm(values, gain, width, power_sum):
    return values * lax.rsqrt(power_sum / width + 1e-06) * gain


def local(
    resid,
    gain_mix_in,
    u_weight,
    v_weight,
    u_scale,
    v_scale,
    v_gain,
    mix_matrix,
    mix_bias,
    out_weight,
    out_scale,
    gain_mix_out,
    gain_ffn_in,
    up_weight,
    up_scale,
    down_weight,
    down_scale,
    gain_ffn_out,
):
    rows = resid.shape[0]
    part_width = resid.shape[1]
    width = part_width * lax.axis_size("tp")
    lane = lax.axis_index("tp")
    full_rows = lax.all_gather(resid, "tp", axis=1, tiled=True)
    out_scales, down_scales = (
        lax.all_gather(out_scale, "fs", axis=0, tiled=True),
        lax.all_gather(down_scale, "fs", axis=0, tiled=True),
    )
    full_float = full_rows.astype(jnp.float32)
    normed = rms_norm(
        full_float, gain_mix_in, width, jnp.sum(full_float * full_float, axis=1, keepdims=True)
    ).astype(jnp.bfloat16)
    branch_cols = u_weight.shape[1]
    u_pre = jnp.dot(
        normed,
        lax.all_gather(u_weight.astype(jnp.bfloat16), "fs", axis=0, tiled=True),
        preferred_element_type=jnp.float32,
    )
    v_pre = jnp.dot(
        normed,
        lax.all_gather(v_weight.astype(jnp.bfloat16), "fs", axis=0, tiled=True),
        preferred_element_type=jnp.float32,
    )
    u_act = jax.nn.gelu(u_pre * u_scale)
    v_act = jax.nn.gelu(v_pre * v_scale)
    total, squares = lax.psum(
        (jnp.sum(v_act, axis=1, keepdims=True), jnp.sum(v_act * v_act, axis=1, keepdims=True)), "tp"
    )
    branch_width = branch_cols * lax.axis_size("tp")
    centre = total / branch_width
    spread = squares / branch_width - centre * centre
    v_norm = ((v_act - centre) * lax.rsqrt(spread + 1e-06) * v_gain).astype(jnp.bfloat16)
    groups = mix_matrix.shape[0]
    block = mix_matrix.shape[1]
    blocks = v_norm.reshape(rows // block, block, groups, branch_cols // groups)
    mixed = (
        jnp.einsum(
            "gts,bsgd->btgd",
            mix_matrix.astype(jnp.bfloat16),
            blocks,
            preferred_element_type=jnp.float32,
        )
        + mix_bias.T[None, :, :, None]
    )
    gated = (u_act * mixed.reshape(rows, branch_cols)).astype(jnp.bfloat16)
    partial_value = jnp.dot(
        gated,
        lax.all_gather(out_weight.astype(jnp.bfloat16), "fs", axis=1, tiled=True),
        preferred_element_type=jnp.float32,
    )
    mix_out = lax.psum(partial_value.astype(jnp.bfloat16), "tp").astype(jnp.float32) * out_scales
    power = jnp.sum(mix_out * mix_out, axis=1, keepdims=True)
    middle_full = (full_float + rms_norm(mix_out, gain_mix_out, width, power)).astype(jnp.bfloat16)
    middle = lax.dynamic_slice_in_dim(middle_full, lane * part_width, part_width, 1)
    middle_float = middle_full.astype(jnp.float32)
    ffn_in = rms_norm(
        middle_float,
        gain_ffn_in,
        width,
        jnp.sum(middle_float * middle_float, axis=1, keepdims=True),
    ).astype(jnp.bfloat16)
    up_half = up_weight.astype(jnp.bfloat16)
    down_half = down_weight.astype(jnp.bfloat16)
    whole_up = lax.all_gather(up_half, "fs", axis=0, tiled=True)
    raised = jnp.dot(ffn_in, whole_up, preferred_element_type=jnp.float32)
    hidden = jnp.square(jax.nn.relu(raised * up_scale)).astype(jnp.bfloat16)
    whole_down = lax.all_gather(down_half, "fs", axis=1, tiled=True)
    terms = jnp.dot(hidden, whole_down, preferred_element_type=jnp.float32)
    own_down = lax.dynamic_slice_in_dim(down_scales, lane * part_width, part_width, 0)
    ffn_out = (
        lax.psum_scatter(terms.astype(jnp.bfloat16), "tp", scatter_dimension=1, tiled=True).astype(
            jnp.float32
        )
        * own_down
    )
    power_out = lax.psum(jnp.sum(ffn_out * ffn_out, axis=1, keepdims=True), "tp")
    own_gain_out = lax.dynamic_slice_in_dim(gain_ffn_out, lane * part_width, part_width, 0)
    return (middle.astype(jnp.float32) + rms_norm(ffn_out, own_gain_out, width, power_out)).astype(
        jnp.bfloat16
    )


def local_fast(
    resid,
    gain_mix_in,
    u_weight,
    v_weight,
    u_scale,
    v_scale,
    v_gain,
    mix_matrix,
    mix_bias,
    out_weight,
    out_scale,
    gain_mix_out,
    gain_ffn_in,
    up_weight,
    up_scale,
    down_weight,
    down_scale,
    gain_ffn_out,
):
    rows, part = resid.shape
    members = lax.axis_size("fs")
    width = part * 2
    depth, branch = v_weight.shape
    shared = up_weight.shape[1] // 2
    parts = 3 + 2 * (shared // branch)
    n_in = 2
    n_out = members // n_in
    half, single = jnp.bfloat16, jnp.float32
    groups, block = mix_matrix.shape[0], mix_matrix.shape[1]

    def row(vector):
        return vector.reshape(1, -1)

    big = [resid, v_weight, u_weight, out_weight, up_weight, down_weight]
    small = [
        row(gain_mix_in),
        row(u_scale),
        row(v_scale),
        row(v_gain),
        mix_matrix,
        mix_bias,
        row(out_scale),
        row(gain_mix_out),
        row(gain_ffn_in),
        row(up_scale),
        row(down_scale),
        row(gain_ffn_out),
    ]
    dma = pltpu.SemaphoreType.DMA
    scratch = [
        pltpu.VMEM((parts, members, depth, branch), half),
        pltpu.VMEM((rows, part), single),
        pltpu.VMEM((rows, width), half),
        pltpu.VMEM((rows, width), half),
        pltpu.VMEM((2, rows, part), half),
        pltpu.VMEM((2, rows, shared), half),
        pltpu.VMEM((2, rows, width), half),
        pltpu.VMEM((rows, width), half),
        pltpu.VMEM((2, rows, part), half),
        pltpu.VMEM((rows, part), half),
        pltpu.VMEM((rows, 128), single),
        pltpu.VMEM((2, rows, 128), single),
        pltpu.VMEM((groups * block, block), half),
        pltpu.VMEM((block, branch), single),
        dma((parts, 2, n_out)),
        dma((parts, n_out)),
        dma((parts - 3, 2, n_out)),
        dma((parts - 3, n_out)),
        dma((parts, n_out)),
        dma((parts, n_out)),
        dma((3, n_out, 2)),
        dma((3, n_out, 2)),
        dma((parts, branch // depth)),
        dma((2,)),
        dma((2,)),
        dma((n_out, 2)),
        dma((n_out, 2)),
        dma((n_out, 2)),
        dma((n_out, 2)),
        dma((3, n_out)),
        dma((3, n_out)),
        dma((n_out, 2)),
        dma((n_out, 2)),
        dma((n_out,)),
    ]
    return pl.pallas_call(
        functools.partial(fused_kernel, n_out, n_in),
        out_shape=jax.ShapeDtypeStruct((rows, part), half),
        in_specs=[pl.BlockSpec(memory_space=pl.ANY)] * len(big)
        + [pl.BlockSpec(memory_space=pltpu.VMEM)] * len(small),
        out_specs=pl.BlockSpec(memory_space=pl.ANY),
        scratch_shapes=scratch,
        compiler_params=pltpu.CompilerParams(
            collective_id=0, has_side_effects=True, vmem_limit_bytes=63 * 1024 * 1024
        ),
        name="fused_layer",
    )(*big, *small)


def solution(mesh):
    in_specs = (
        P(("rep", "fs"), "tp"),
        P(),
        P("fs", "tp"),
        P("fs", "tp"),
        P("tp"),
        P("tp"),
        P("tp"),
        P("tp", None, None),
        P("tp", None),
        P("tp", "fs"),
        P("fs"),
        P(),
        P(),
        P("fs", "tp"),
        P("tp"),
        P("tp", "fs"),
        P("fs"),
        P(),
    )
    out_specs = P(("rep", "fs"), "tp")
    sizes = mesh.shape

    def whole(*args):
        rows = args[0].shape[0] // (sizes["rep"] * sizes["fs"])
        width = args[0].shape[1]
        branch = args[2].shape[1] // sizes["tp"]
        hidden = args[13].shape[1] // sizes["tp"]
        groups, block = args[7].shape[0] // sizes["tp"], args[7].shape[1]
        planes, depth = sizes["fs"] // 2, width // sizes["fs"]
        paired = sizes["rep"] == 2 and sizes["tp"] == 2 and sizes["fs"] % 4 == 0
        fits = depth % 256 == 0 and branch % depth == 0 and hidden == 4 * branch
        blocks = rows % (planes * block) == 0 and (256 * groups) % branch == 0
        small = 2 * width * (3 * branch + 2 * hidden) <= 24 * 1024 * 1024
        fast = paired and planes == 4 and fits and blocks and small
        return mapped(local_fast if fast else local)(*args)

    def mapped(body):
        return jax.shard_map(
            body, mesh=mesh, in_specs=in_specs, out_specs=out_specs, check_vma=False
        )

    return whole
```
